512 devices in a mesh: sp: 64 (over z, y), tp: 8 (over x, core).
Axes of the slice: x: 4, y: 4, z: 16, core: 2. Of those that a mesh axis runs over, the one named last changes fastest.
Arguments:
- stream: bfloat16 [24576, 2048], P('sp'), may hold values from -40 to 40
- query_rows: bfloat16 [24576, 1024], P('sp', 'tp'), may hold values from -10 to 10
- key_rows: bfloat16 [24576, 256], P('sp'), may hold values from -10 to 10
- value_rows: bfloat16 [24576, 256], P('sp'), may hold values from -6 to 6
- doc_ids: int32 [24576], P('sp'), may hold values from 0 to 31, never falling along the last dimension, each value on 1 to 1536 neighbouring positions
- sink_logit: float32 [8], P('tp'), may hold values from 2 to 7
- out_weight: bfloat16 [1024, 2048], P('tp'), may hold values from -1.5 to 1.5
- norm_gain: float32 [2048], replicated, may hold values from 0.1 to 1.9
- gate_weight: bfloat16 [2048, 5632], P('sp', 'tp'), may hold values from -0.125 to 0.125
- up_weight: bfloat16 [2048, 5632], P('sp', 'tp'), may hold values from -0.125 to 0.125
- down_weight: bfloat16 [5632, 2048], P('tp', 'sp'), may hold values from -0.078125 to 0.078125
Outputs:
- mixed_out: bfloat16 [24576, 2048], P('sp')
The draws below stay inside these ranges and needn't reach their ends.
Inputs may be any that keep to these rules, and one draw needn't show every extreme that they name: `doc_ids`: document numbers never fall along the sequence; each document has 1 to 1536 positions.
All inputs are finite; a program needn't handle non-finite values.
Results may differ from the reference program's by a relative error of at most 0.009.
Values may be sent and summed in bfloat16 or wider, within the bound.
A program may use at most 64 MiB of HBM per device.

```python
import math
import jax
import jax.numpy as jnp
import numpy as np
from jax import lax

D = 2048
FF = 5632
HEADS = 8
KVH = 2
HD = 128
WIN = 128
TOK_DEV = 384
TOKENS = 24576
DOCS = 32
DOC_MOST = 1536
N_TP = 8


def draw_stream(key, part):
    first_key, second_key = jax.random.split(key, 2)
    column_scale = 3.0 ** (jnp.arange(D, dtype=jnp.float32) / D)
    base = jnp.clip(jax.random.normal(first_key, (TOKENS, D), jnp.float32), -6.0, 6.0)
    row_scale = jnp.exp(jax.random.uniform(second_key, (TOKENS, 1), jnp.float32, -0.7, 0.7))
    values = base * row_scale * column_scale[None, :]
    return values.astype(jnp.bfloat16)


def draw_query_rows(key, part):
    values = jnp.clip(jax.random.normal(jax.random.fold_in(key, 1), (TOKENS, HEADS * HD), jnp.float32), -6.0, 6.0)
    return values.astype(jnp.bfloat16)


def draw_key_rows(key, part):
    values = jnp.clip(jax.random.normal(jax.random.fold_in(key, 2), (TOKENS, KVH * HD), jnp.float32), -6.0, 6.0)
    return values.astype(jnp.bfloat16)


def block_levels(stream_key, dims, pieces, least, largest):
    def one(dim, blocks):
        heights = jax.random.uniform(jax.random.fold_in(jax.random.fold_in(stream_key, 6), dim), (blocks,), jnp.float32, least / len(pieces), largest / len(pieces))
        return jnp.repeat(jnp.exp(heights), dims[dim] // blocks).reshape((-1,) + (1,) * (len(dims) - dim - 1))

    loudness = one(*pieces[0])
    for cut in pieces[1:]:
        loudness = loudness * one(*cut)
    return loudness


def profile(count, total, reach, slope):
    portions = [(1 << 20) // math.isqrt(rank ** slope) + 1 for rank in range(2, count + 1)]
    surplus, holding = total - reach - (count - 1), [1] * (count - 1)
    while surplus > 0:
        free = [i for i in range(count - 1) if holding[i] < reach]
        whole, remaining = sum([portions[i] for i in free]), surplus
        for i in free:
            more = min(reach - holding[i], max(1, remaining * portions[i] // whole), surplus)
            holding[i] = holding[i] + more
            surplus = surplus - more
    return np.array([reach] + holding)


def uneven_parts(rng, count, total, limit, skew):
    if count == 2:
        one = jax.random.randint(rng, (), max(1, total - limit), min(limit, total - 1) + 1)
        return jnp.stack([one, total - one])
    lengths = jnp.asarray(profile(count, total, limit, skew), jnp.int32)
    couples = (count - 1) // 2
    source_of, sink = lengths[1:1 + 2 * couples:2], lengths[2:2 + 2 * couples:2]
    room = jnp.minimum(source_of - 1, limit - sink)
    passed = jax.random.randint(jax.random.fold_in(rng, 1), (couples,), 0, 1 << 20) % (room + 1)
    lengths = lengths.at[1:1 + 2 * couples:2].set(source_of - passed).at[2:2 + 2 * couples:2].set(sink + passed)
    return lengths[jax.random.permutation(jax.random.fold_in(rng, 2), count)]


def noise(own_key, shape, scale, bound, cuts=(), kind=jnp.bfloat16):
    level = block_levels(own_key, shape, cuts, -0.22, 0.18) if cuts else 1.0
    entries = jax.random.normal(own_key, shape, jnp.float32) * scale * level
    return jnp.minimum(jnp.maximum(entries, -bound), bound).astype(kind)


def setup_inputs(seed: int = 0) -> dict:
    splits = jax.random.split(jax.random.key(seed), 12)
    return {
        "stream": draw_stream(jax.random.fold_in(splits[11], 71), 0),
        "query_rows": draw_query_rows(jax.random.fold_in(splits[11], 71), 0),
        "key_rows": draw_key_rows(jax.random.fold_in(splits[11], 71), 0),
        "value_rows": noise(splits[3], (TOKENS, KVH * HD), 1.0, 6.0, ((0, 64),)),
        "doc_ids": jnp.searchsorted(jnp.cumsum(uneven_parts(splits[4], DOCS, TOKENS, DOC_MOST, 1)), jnp.arange(TOKENS), side="right").astype(jnp.int32),
        "sink_logit": jnp.clip(2.0 + 5.0 * jax.random.uniform(splits[5], (HEADS,), jnp.float32) ** block_levels(splits[5], (HEADS,), ((0, 8),), -0.2, 0.2), 2.0, 7.0),
        "out_weight": noise(splits[6], (HEADS * HD, D), (HEADS * HD // 64) ** -0.5, 1.5, ((0, 8),)),
        "norm_gain": jnp.clip(1.0 + 0.18 * jax.random.normal(splits[7], (D,), jnp.float32), 0.1, 1.9),
        "gate_weight": noise(splits[8], (D, FF), D ** -0.5, 0.125, ((0, 64), (1, 8))),
        "up_weight": noise(splits[9], (D, FF), D ** -0.5, 0.125, ((0, 64), (1, 8))),
        "down_weight": noise(splits[10], (FF, D), FF ** -0.5, 0.078125, ((0, 8), (1, 64))),
    }


norm_eps = 1e-06
masked_low = -1e+30

def reference(stream, query_rows, key_rows, value_rows, doc_ids, sink_logit, out_weight, norm_gain, gate_weight, up_weight, down_weight):
    seq_total = stream.shape[0]
    group_share = HEADS // KVH
    keys_pad = jnp.pad(key_rows, ((WIN, WIN), (0, 0)))
    values_pad = jnp.pad(value_rows, ((WIN, WIN), (0, 0)))
    docs_pad = jnp.pad(doc_ids, (WIN, WIN))
    head_block = HEADS * HD // N_TP
    ff_block = FF // N_TP
    span = TOK_DEV + 2 * WIN

    def one_block(block_id):
        begin_at = (block_id * TOK_DEV).astype(jnp.int32)
        queries = lax.dynamic_slice_in_dim(query_rows, begin_at, TOK_DEV, 0).astype(jnp.float32).reshape(TOK_DEV, KVH, group_share, HD)
        keys_grid = lax.dynamic_slice_in_dim(keys_pad, begin_at, span, 0).astype(jnp.float32).reshape(span, KVH, HD)
        values_grid = lax.dynamic_slice_in_dim(values_pad, begin_at, span, 0).astype(jnp.float32).reshape(span, KVH, HD)
        docs_here = lax.dynamic_slice_in_dim(doc_ids, begin_at, TOK_DEV, 0)
        docs_wide = lax.dynamic_slice_in_dim(docs_pad, begin_at, span, 0)
        query_pos = begin_at + jnp.arange(TOK_DEV, dtype=jnp.int32)
        key_pos = begin_at - WIN + jnp.arange(span, dtype=jnp.int32)
        allowed = (jnp.abs(query_pos[:, None] - key_pos[None, :]) <= WIN) & (key_pos[None, :] >= 0) & (key_pos[None, :] < seq_total) & (docs_here[:, None] == docs_wide[None, :])
        scores = jnp.einsum('qgrd,kgd->grqk', queries, keys_grid) * HD ** (-0.5)
        masked = jnp.where(allowed[None, None], scores, masked_low)
        sinks = sink_logit.astype(jnp.float32).reshape(KVH, group_share, 1, 1)
        peak = jnp.maximum(lax.optimization_barrier(jnp.max(masked, axis=-1, keepdims=True)), sinks)
        lifted = jnp.where(allowed[None, None], jnp.exp(masked - peak), 0.0)
        denom = lax.optimization_barrier(jnp.sum(lifted, axis=-1, keepdims=True)) + jnp.exp(sinks - peak)
        probs = (lifted / denom).astype(jnp.bfloat16)
        attended = jnp.einsum('grqk,kgd->qgrd', probs.astype(jnp.float32), values_grid)
        attended = attended.astype(jnp.bfloat16).reshape(TOK_DEV, HEADS * HD)
        branch_sum = jnp.zeros((TOK_DEV, D), jnp.float32)
        for part_id in range(N_TP):
            term = jnp.dot(attended[:, part_id * head_block:(part_id + 1) * head_block], out_weight[part_id * head_block:(part_id + 1) * head_block], preferred_element_type=jnp.float32)
            branch_sum = branch_sum + lax.optimization_barrier(term.astype(jnp.bfloat16)).astype(jnp.float32)
        branch = branch_sum.astype(jnp.bfloat16)
        stream_here = lax.dynamic_slice_in_dim(stream, begin_at, TOK_DEV, 0)
        carried = (stream_here.astype(jnp.float32) + branch.astype(jnp.float32)).astype(jnp.bfloat16)
        carried_f = carried.astype(jnp.float32)
        normed = (carried_f * lax.rsqrt(lax.optimization_barrier(jnp.mean(carried_f * carried_f, axis=1, keepdims=True)) + norm_eps) * norm_gain.astype(jnp.float32)).astype(jnp.bfloat16)
        gate_acc = jnp.dot(normed, gate_weight, preferred_element_type=jnp.float32)
        up_acc = jnp.dot(normed, up_weight, preferred_element_type=jnp.float32)
        hidden = (jax.nn.silu(gate_acc) * up_acc).astype(jnp.bfloat16)
        feed_sum = jnp.zeros((TOK_DEV, D), jnp.float32)
        for part_id in range(N_TP):
            term = jnp.dot(hidden[:, part_id * ff_block:(part_id + 1) * ff_block], down_weight[part_id * ff_block:(part_id + 1) * ff_block], preferred_element_type=jnp.float32)
            feed_sum = feed_sum + lax.optimization_barrier(term.astype(jnp.bfloat16)).astype(jnp.float32)
        feed = feed_sum.astype(jnp.bfloat16)
        return (carried_f + 0.5 * feed.astype(jnp.float32)).astype(jnp.bfloat16)
    blocks_all = lax.map(one_block, jnp.arange(seq_total // TOK_DEV, dtype=jnp.int32))
    return blocks_all.reshape(seq_total, D)
```

```python
import jax
import jax.numpy as jnp
from jax import lax
from jax.experimental import pallas as pl
from jax.experimental.pallas import tpu as pltpu
from jax.sharding import Mesh
from jax.sharding import PartitionSpec as P

HD = 128
WIN = 128
NZ, NY, NX, NC = 16, 4, 4, 2
TOK = 384
D = 2048
FFL = 704
MAIN = 640
TAIL = 64
GU = 2 * FFL
FP = 768
OWN = TOK // (NX * NC)
EPS = 1e-06
LOW = -1e30
COPIES = 140
SP = ("z", "y")
TP = ("x", "c")
F32 = jnp.float32
BF = jnp.bfloat16


def kernel(
    stream,
    query,
    key,
    value,
    doc_col,
    doc_row,
    sink,
    out_w,
    gain,
    gu,
    dn,
    out,
    kext,
    vext,
    dext,
    wg,
    wd,
    ow,
    att,
    carried,
    normed,
    acc,
    hid,
    part,
    summed,
    pair_in,
    opp_in,
    relay,
    near_in,
    far_in,
    send_sems,
    recv_sems,
):
    z, y = lax.axis_index("z"), lax.axis_index("y")
    x, c = lax.axis_index("x"), lax.axis_index("c")
    zr, zl = lax.rem(z + 1, NZ), lax.rem(z + NZ - 1, NZ)
    yr, yl = lax.rem(y + 1, NY), lax.rem(y + NY - 1, NY)
    xr, xl = lax.rem(x + 1, NX), lax.rem(x + NX - 1, NX)
    yo, xo = lax.rem(y + 2, NY), lax.rem(x + 2, NX)
    pc = 1 - c
    sp = z * NY + y
    after, before = lax.rem(sp + 1, NZ * NY), lax.rem(sp + NZ * NY - 1, NZ * NY)
    dev_zr, dev_zl = (zr, y, x, c), (zl, y, x, c)
    dev_yr, dev_yl = (z, yr, x, c), (z, yl, x, c)
    dev_xr, dev_xl = (z, y, xr, c), (z, y, xl, c)
    dev_p = (z, y, x, pc)
    dev_after = (after // NY, lax.rem(after, NY), x, c)
    dev_before = (before // NY, lax.rem(before, NY), x, c)

    barrier = pltpu.get_barrier_semaphore()
    peers = (dev_zr, dev_zl, dev_yr, dev_yl, dev_xr, dev_xl, dev_p, dev_after, dev_before)
    for peer in peers:
        pl.semaphore_signal(barrier, inc=1, device_id=peer, device_id_type=pl.DeviceIdType.MESH)
    pl.semaphore_wait(barrier, len(peers))

    started = []

    def send(src, dst, dev):
        at = len(started)
        copy = pltpu.make_async_remote_copy(
            src_ref=src,
            dst_ref=dst,
            send_sem=send_sems.at[at],
            recv_sem=recv_sems.at[at],
            device_id=dev,
            device_id_type=pl.DeviceIdType.MESH,
        )
        copy.start()
        started.append(copy)
        return copy

    def zm(s):
        return lax.rem(z + NZ - s, NZ)

    def zp(s):
        return lax.rem(z + s, NZ)

    g_zl, g_zr, g_yl, g_yr, g_yo = {}, {}, {}, {}, {}

    def g_to_y(src, at, tag):
        g_yl[tag] = send(src, wg.at[at, y], dev_yr)
        g_yr[tag] = send(src, wg.at[at, y], dev_yl)

    def g_start():
        g_zl[0] = send(gu, wg.at[z, y], dev_zr)
        g_zr[0] = send(gu, wg.at[z, y], dev_zl)
        g_to_y(gu, z, (0, 0))

    def tags(s):
        if s == 0:
            return [(0, 0)]
        if s == 8:
            return [(0, 8)]
        return [(0, s), (1, s)]

    def place(tag):
        return zm(tag[1]) if tag[0] == 0 else zp(tag[1])

    def g_ring(s):
        g_zl[s - 1].wait_recv()
        at = zm(s)
        if s < 8:
            g_zl[s] = send(wg.at[at, y], wg.at[at, y], dev_zr)
        if s <= 7:
            g_zr[s - 1].wait_recv()
            other = zp(s)
            if s < 7:
                g_zr[s] = send(wg.at[other, y], wg.at[other, y], dev_zl)
        for tag in tags(s):
            at = place(tag)
            g_to_y(wg.at[at, y], at, tag)

    def g_across(s):
        for tag in tags(s):
            at = place(tag)
            rightward = (tag[0] == 0 and tag[1] < 8)
            g_yl[tag].wait_recv()
            if rightward:
                g_yo[tag] = send(wg.at[at, yl], wg.at[at, yl], dev_yr)
            g_yr[tag].wait_recv()
            if not rightward:
                g_yo[tag] = send(wg.at[at, yr], wg.at[at, yr], dev_yl)

    def g_done(s):
        for tag in tags(s):
            g_yo[tag].wait_recv()

    d_y, d_zl, d_zr = {}, {}, {}

    def d_start():
        d_y["l"] = send(dn, wd.at[z, y], dev_yr)
        d_y["r"] = send(dn, wd.at[z, y], dev_yl)

    def d_forward():
        d_y["l"].wait_recv()
        d_y["o"] = send(wd.at[z, yl], wd.at[z, yl], dev_yr)
        d_y["r"].wait_recv()

    def d_begin():
        d_y["o"].wait_recv()
        d_zl[0] = send(wd.at[z], wd.at[z], dev_zr)
        d_zr[0] = send(wd.at[z], wd.at[z], dev_zl)

    def d_ring(s):
        d_zl[s - 1].wait_recv()
        if s < 8:
            at = zm(s)
            d_zl[s] = send(wd.at[at], wd.at[at], dev_zr)
        if s <= 7:
            d_zr[s - 1].wait_recv()
            if s < 7:
                other = zp(s)
                d_zr[s] = send(wd.at[other], wd.at[other], dev_zl)

    def x_start(src, slot):
        own = slot(x, c)
        return {"l": send(src, own, dev_xr), "r": send(src, own, dev_xl), "p": send(src, own, dev_p)}

    def x_forward(g, slot, halves):
        left, right = slot(xl, c), slot(xr, c)
        g["l"].wait_recv()
        g["a"] = send(halves(left)[0], halves(left)[0], dev_xr)
        g["pl"] = send(left, left, dev_p)
        g["r"].wait_recv()
        g["b"] = send(halves(right)[1], halves(right)[1], dev_xl)
        g["pr"] = send(right, right, dev_p)

    def x_relay(g, slot, halves):
        a, b = halves(slot(xo, c))
        g["a"].wait_recv()
        g["pa"] = send(a, a, dev_p)
        g["b"].wait_recv()
        g["pb"] = send(b, b, dev_p)

    def x_done(g):
        for name in ("p", "pl", "pr", "pa", "pb"):
            g[name].wait_recv()

    def ow_slot(a, b):
        return ow.at[a * NC + b]

    def ow_halves(ref):
        return ref.at[pl.ds(0, 64)], ref.at[pl.ds(64, 64)]

    def att_slot(a, b):
        return att.at[a * NC + b]

    def att_halves(ref):
        return ref.at[pl.ds(0, 192)], ref.at[pl.ds(192, 192)]

    def out_slot(a, b):
        return out.at[b * NX + a]

    def lane_halves(ref):
        return ref.at[:, pl.ds(0, D // 2)], ref.at[:, pl.ds(D // 2, D // 2)]

    group = pl.multiple_of((x // 2) * HD, HD)
    lanes = pl.ds(group, HD)
    g_start()
    d_start()
    halo = [
        send(key.at[pl.ds(256, 128), lanes], kext.at[pl.ds(0, 128)], dev_after),
        send(value.at[pl.ds(256, 128), lanes], vext.at[pl.ds(0, 128)], dev_after),
        send(doc_row.at[2], dext.at[0], dev_after),
        send(key.at[pl.ds(0, 128), lanes], kext.at[pl.ds(512, 128)], dev_before),
        send(value.at[pl.ds(0, 128), lanes], vext.at[pl.ds(512, 128)], dev_before),
        send(doc_row.at[0], dext.at[1], dev_before),
    ]
    ow_g = x_start(out_w, ow_slot)
    kext[pl.ds(128, 384), :] = key[:, lanes]
    vext[pl.ds(128, 384), :] = value[:, lanes]
    wg[z, y] = gu[...]
    wd[z, y] = dn[...]
    ow[x * NC + c] = out_w[...]
    d_forward()

    for copy in halo:
        copy.wait_recv()
    d_begin()

    def attend(block):
        q = query[pl.ds(block * 128, 128), :]
        k = kext[pl.ds(block * 128, 384), :]
        v = vext[pl.ds(block * 128, 384), :]
        scores = lax.dot_general(q, k, (((1,), (1,)), ((), ())), preferred_element_type=F32)
        scores = scores * HD ** (-0.5)
        if block == 0:
            first = jnp.where(sp == 0, -1, dext[0, 0:1])
        else:
            first = doc_row[block - 1, 0:1]
        if block == 2:
            last = jnp.where(sp == NZ * NY - 1, -1, dext[1, 0:1])
        else:
            last = doc_row[block + 1, 0:1]
        docs = jnp.concatenate([first, doc_row[block, 0:1], last], axis=1)
        mine = doc_col[pl.ds(block * 128, 128), :]
        row = lax.broadcasted_iota(jnp.int32, (128, 384), 0)
        col = lax.broadcasted_iota(jnp.int32, (128, 384), 1)
        allowed = (col >= row) & (col <= row + 2 * WIN) & (mine == docs)
        masked = jnp.where(allowed, scores, LOW)
        here = sink[0]
        peak = jnp.maximum(jnp.max(masked, axis=1, keepdims=True), here)
        lifted = jnp.where(allowed, jnp.exp(masked - peak), 0.0)
        denom = jnp.sum(lifted, axis=1, keepdims=True) + jnp.exp(here - peak)
        probs = (lifted / denom).astype(BF)
        attended = jnp.dot(probs, v, preferred_element_type=F32).astype(BF)
        att[x * NC + c, pl.ds(block * 128, 128), :] = attended

    attend(0)
    g_ring(1)
    attend(1)
    attend(2)
    g_across(0)
    d_ring(1)
    g_ring(2)
    att_g = x_start(att.at[x * NC + c], att_slot)
    g_across(1)
    d_ring(2)
    x_forward(ow_g, ow_slot, ow_halves)
    g_ring(3)
    g_across(2)
    x_forward(att_g, att_slot, att_halves)
    d_ring(3)
    g_ring(4)
    g_across(3)
    x_relay(ow_g, ow_slot, ow_halves)
    x_relay(att_g, att_slot, att_halves)
    d_ring(4)
    x_done(ow_g)
    x_done(att_g)

    def project(n, squares):
        cols = pl.ds(pl.multiple_of(n * 256, 256), 256)
        left = jnp.concatenate([att[h] for h in range(8)], axis=1)
        right = ow[:, :, cols].reshape(1024, 256)
        branch = jnp.dot(left, right, preferred_element_type=F32).astype(BF)
        total = (stream[:, cols].astype(F32) + branch.astype(F32)).astype(BF)
        carried[:, :, cols] = total.reshape(8, OWN, 256)
        wide = total.astype(F32)
        return squares + jnp.sum(wide * wide, axis=1, keepdims=True)

    squares = lax.fori_loop(0, 8, project, jnp.zeros((TOK, 1), F32))
    scale = lax.rsqrt(squares / D + EPS)

    g_ring(5)

    def normalize(n, carry):
        cols = pl.ds(pl.multiple_of(n * 256, 256), 256)
        wide = carried[:, :, cols].reshape(TOK, 256).astype(F32)
        normed[:, cols] = (wide * scale * gain[:, cols]).astype(BF)
        return carry

    lax.fori_loop(0, 8, normalize, 0)
    g_across(4)
    d_ring(5)
    g_ring(6)

    def accumulate(za, zb, first):
        left = jnp.concatenate(
            [
                normed[:, pl.ds(pl.multiple_of(za * 128, 128), 128)],
                normed[:, pl.ds(pl.multiple_of(zb * 128, 128), 128)],
            ],
            axis=1,
        )
        for lo, size in ((0, 512), (512, 512), (1024, 384)):
            cols = pl.ds(lo, size)
            right = jnp.concatenate(
                [wg[za, :, :, cols].reshape(128, size), wg[zb, :, :, cols].reshape(128, size)], axis=0
            )
            term = jnp.dot(left, right, preferred_element_type=F32)
            if first:
                acc[:, cols] = term
            else:
                acc[:, cols] += term

    def accumulate_tag(s, first=False):
        accumulate(zm(s), zp(s), first)

    g_done(1)
    accumulate_tag(1, True)
    g_across(5)
    d_ring(6)
    g_done(2)
    g_done(3)

    def both(i, carry):
        accumulate_tag(i)
        return carry

    lax.fori_loop(2, 4, both, 0)
    g_ring(7)
    g_across(6)
    d_ring(7)
    g_done(4)
    accumulate_tag(4)
    g_ring(8)
    g_across(7)
    d_ring(8)
    g_done(5)
    accumulate_tag(5)
    g_across(8)
    g_done(6)
    accumulate_tag(6)
    g_done(7)
    accumulate_tag(7)
    g_done(0)
    g_done(8)
    accumulate(z, zm(8), False)

    gate, up = acc[:, 0:MAIN], acc[:, MAIN : 2 * MAIN]
    hid[:, 0:MAIN] = (gate / (1.0 + jnp.exp(-gate)) * up).astype(BF)
    rest = acc[:, 2 * MAIN : GU]
    swapped = pltpu.roll(rest, TAIL, 1)
    tail = (rest / (1.0 + jnp.exp(-rest)) * swapped).astype(BF)
    lane = lax.broadcasted_iota(jnp.int32, (TOK, 2 * TAIL), 1)
    hid[:, MAIN:FP] = jnp.where(lane < TAIL, tail.astype(F32), 0.0).astype(BF)

    def lower(n, carry):
        w = wd[pl.ds(2 * n, 2)].reshape(256, FP)
        term = lax.dot_general(hid[...], w, (((1,), (1,)), ((), ())), preferred_element_type=F32)
        cols = pl.ds(pl.multiple_of(n * 256, 256), 256)
        part[:, :, :, cols] = term.astype(BF).reshape(NC, NX, OWN, 256)
        return carry

    lax.fori_loop(0, 8, lower, 0)

    to_pair = send(part.at[pc], pair_in, dev_p)
    to_pair.wait_recv()

    def fold(i, carry):
        at = lax.rem(xo + i, NX)
        summed[at] = (part[c, at].astype(F32) + pair_in[at].astype(F32)).astype(BF)
        return carry

    lax.fori_loop(0, 4, fold, 0)
    half = D // 2
    low, high = pl.ds(0, half), pl.ds(half, half)
    opp_a = send(summed.at[xo, :, low], opp_in.at[0], dev_xr)
    opp_b = send(summed.at[xo, :, high], opp_in.at[1], dev_xl)
    near_b = send(summed.at[xr, :, high], near_in.at[1], dev_xr)
    near_a = send(summed.at[xl, :, low], near_in.at[0], dev_xl)
    opp_a.wait_recv()
    relay[0] = (opp_in[0].astype(F32) + summed[xr, :, low].astype(F32)).astype(BF)
    opp_b.wait_recv()
    relay[1] = (opp_in[1].astype(F32) + summed[xl, :, high].astype(F32)).astype(BF)
    far_a = send(relay.at[0], far_in.at[0], dev_xr)
    far_b = send(relay.at[1], far_in.at[1], dev_xl)
    near_a.wait_recv()
    near_b.wait_recv()
    own = c * NX + x
    for i, arrived in ((0, far_a), (1, far_b)):
        arrived.wait_recv()
        cols = pl.ds(i * half, half)
        feed = summed[x, :, cols].astype(F32) + near_in[i].astype(F32) + far_in[i].astype(F32)
        feed = feed.astype(BF).astype(F32)
        out[own, :, cols] = (carried[own, :, cols].astype(F32) + 0.5 * feed).astype(BF)
    out_g = x_start(out.at[own], out_slot)
    x_forward(out_g, out_slot, lane_halves)
    x_relay(out_g, out_slot, lane_halves)
    x_done(out_g)
    for copy in started:
        copy.wait_send()


def per_device(
    stream,
    query_rows,
    key_rows,
    value_rows,
    doc_ids,
    sink_logit,
    out_weight,
    norm_gain,
    gate_weight,
    up_weight,
    down_weight,
):
    gu = jnp.concatenate(
        [gate_weight[:, :MAIN], up_weight[:, :MAIN], gate_weight[:, MAIN:], up_weight[:, MAIN:]], axis=1
    )
    dn = jnp.pad(down_weight.T, ((0, 0), (0, FP - FFL)))
    doc_col = doc_ids.reshape(TOK, 1)
    doc_row = jnp.broadcast_to(doc_ids.reshape(3, 1, 128), (3, 8, 128))
    vmem = pl.BlockSpec(memory_space=pltpu.VMEM)
    smem = pl.BlockSpec(memory_space=pltpu.SMEM)
    result = pl.pallas_call(
        kernel,
        out_shape=jax.ShapeDtypeStruct((8, OWN, D), BF),
        in_specs=[vmem] * 6 + [smem] + [vmem] * 4,
        out_specs=vmem,
        scratch_shapes=[
            pltpu.VMEM((TOK + 2 * WIN, HD), BF),
            pltpu.VMEM((TOK + 2 * WIN, HD), BF),
            pltpu.VMEM((2, 8, 128), jnp.int32),
            pltpu.VMEM((NZ, NY, 32, GU), BF),
            pltpu.VMEM((NZ, NY, 32, FP), BF),
            pltpu.VMEM((8, 128, D), BF),
            pltpu.VMEM((8, TOK, HD), BF),
            pltpu.VMEM((8, OWN, D), BF),
            pltpu.VMEM((TOK, D), BF),
            pltpu.VMEM((TOK, GU), F32),
            pltpu.VMEM((TOK, FP), BF),
            pltpu.VMEM((NC, NX, OWN, D), BF),
            pltpu.VMEM((NX, OWN, D), BF),
            pltpu.VMEM((NX, OWN, D), BF),
            pltpu.VMEM((2, OWN, D // 2), BF),
            pltpu.VMEM((2, OWN, D // 2), BF),
            pltpu.VMEM((2, OWN, D // 2), BF),
            pltpu.VMEM((2, OWN, D // 2), BF),
            pltpu.SemaphoreType.DMA((COPIES,)),
            pltpu.SemaphoreType.DMA((COPIES,)),
        ],
        compiler_params=pltpu.CompilerParams(
            collective_id=0, has_side_effects=True, vmem_limit_bytes=60 * 1024 * 1024
        ),
    )(
        stream,
        query_rows,
        key_rows,
        value_rows,
        doc_col,
        doc_row,
        sink_logit,
        out_weight,
        norm_gain.reshape(1, D),
        gu,
        dn,
    )
    return result.reshape(TOK, D)


def solution(mesh):
    split = Mesh(mesh.devices.reshape(NZ, NY, NX, NC), ("z", "y", "x", "c"))
    placed = (
        P(SP, None),
        P(SP, TP),
        P(SP, None),
        P(SP, None),
        P(SP),
        P(TP),
        P(TP, None),
        P(),
        P(SP, TP),
        P(SP, TP),
        P(TP, SP),
    )
    return jax.shard_map(
        per_device, mesh=split, in_specs=placed, out_specs=P(SP, None), check_vma=False
    )
```

```python
import jax
import jax.numpy as jnp
from jax import lax
from jax.experimental import pallas as pl
from jax.experimental.pallas import tpu as pltpu
from jax.sharding import Mesh
from jax.sharding import PartitionSpec as P

HD = 128
WIN = 128
NZ, NY, NX, NC = 16, 4, 4, 2
TOK = 384
D = 2048
FFL = 704
MAIN = 640
TAIL = 64
FP = 768
OWN = TOK // (NX * NC)
EPS = 1e-06
LOW = -1e30
COPIES = 260
SP = ("z", "y")
TP = ("x", "c")
F32 = jnp.float32
BF = jnp.bfloat16


def kernel(
    stream_far,
    query,
    key,
    value,
    docs,
    sink,
    out_w,
    gain,
    gate_w,
    up_w,
    down_w,
    out,
    stream,
    kext,
    vext,
    dsend,
    dext,
    gb_own,
    dn_own,
    wga,
    wgb,
    wd,
    ow,
    att,
    carried,
    normed,
    acc_a,
    acc_b,
    hid,
    part,
    summed,
    pair_in,
    opp_in,
    relay,
    near_in,
    far_in,
    local_sem,
    send_sems,
    recv_sems,
):
    z, y = lax.axis_index("z"), lax.axis_index("y")
    x, c = lax.axis_index("x"), lax.axis_index("c")
    zr, zl = lax.rem(z + 1, NZ), lax.rem(z + NZ - 1, NZ)
    yr, yl = lax.rem(y + 1, NY), lax.rem(y + NY - 1, NY)
    xr, xl = lax.rem(x + 1, NX), lax.rem(x + NX - 1, NX)
    yo, xo = lax.rem(y + 2, NY), lax.rem(x + 2, NX)
    pc = 1 - c
    sp = z * NY + y
    after, before = lax.rem(sp + 1, NZ * NY), lax.rem(sp + NZ * NY - 1, NZ * NY)
    dev_zr, dev_zl = (zr, y, x, c), (zl, y, x, c)
    dev_yr, dev_yl = (z, yr, x, c), (z, yl, x, c)
    dev_xr, dev_xl = (z, y, xr, c), (z, y, xl, c)
    dev_p = (z, y, x, pc)
    dev_after = (after // NY, lax.rem(after, NY), x, c)
    dev_before = (before // NY, lax.rem(before, NY), x, c)

    barrier = pltpu.get_barrier_semaphore()
    peers = (dev_zr, dev_zl, dev_yr, dev_yl, dev_xr, dev_xl, dev_p, dev_after, dev_before)
    for peer in peers:
        pl.semaphore_signal(barrier, inc=1, device_id=peer, device_id_type=pl.DeviceIdType.MESH)
    stream_copy = pltpu.make_async_copy(stream_far, stream, local_sem)
    stream_copy.start()

    gb_own[:, 0:MAIN] = up_w[:, 0:MAIN]
    gb_own[:, MAIN:FP] = jnp.concatenate([gate_w[:, MAIN:FFL], up_w[:, MAIN:FFL]], axis=1)
    dn_own[:, 0:MAIN] = down_w[:, 0:MAIN]
    dn_own[:, MAIN:FP] = jnp.concatenate([down_w[:, MAIN:FFL], jnp.zeros((32, TAIL), BF)], axis=1)
    dsend[0] = jnp.broadcast_to(docs[2:3], (8, 128))
    dsend[1] = jnp.broadcast_to(docs[0:1], (8, 128))
    group = pl.multiple_of((x // 2) * HD, HD)
    lanes = pl.ds(group, HD)
    kext[pl.ds(128, 384), :] = key[:, lanes]
    vext[pl.ds(128, 384), :] = value[:, lanes]
    wga[z, y] = gate_w[:, 0:MAIN]
    wgb[z, y] = gb_own[...]
    wd[z, y] = dn_own[...]

    pl.semaphore_wait(barrier, len(peers))

    started = []

    def send(src, dst, dev):
        at = len(started)
        copy = pltpu.make_async_remote_copy(
            src_ref=src,
            dst_ref=dst,
            send_sem=send_sems.at[at],
            recv_sem=recv_sems.at[at],
            device_id=dev,
            device_id_type=pl.DeviceIdType.MESH,
        )
        copy.start()
        started.append(copy)
        return copy

    def zm(s):
        return lax.rem(z + NZ - s, NZ)

    def zp(s):
        return lax.rem(z + s, NZ)

    def tags(s):
        if s == 0:
            return [(0, 0)]
        if s == 8:
            return [(0, 8)]
        return [(0, s), (1, s)]

    def place(tag):
        return zm(tag[1]) if tag[0] == 0 else zp(tag[1])

    class ZFirst:
        def __init__(self, own, buf):
            self.own, self.buf = own, buf
            self.left, self.right, self.yl, self.yr, self.yo = {}, {}, {}, {}, {}

        def to_y(self, src, at, tag):
            self.yl[tag] = send(src, self.buf.at[at, y], dev_yr)
            self.yr[tag] = send(src, self.buf.at[at, y], dev_yl)

        def start(self):
            self.left[0] = send(self.own, self.buf.at[z, y], dev_zr)
            self.right[0] = send(self.own, self.buf.at[z, y], dev_zl)
            self.to_y(self.own, z, (0, 0))

        def ring(self, s):
            block = self.buf.at[zm(s), y]
            self.left[s - 1].wait_recv()
            if s < 8:
                self.left[s] = send(block, block, dev_zr)
            if s <= 7:
                block = self.buf.at[zp(s), y]
                self.right[s - 1].wait_recv()
                if s < 7:
                    self.right[s] = send(block, block, dev_zl)
            for tag in tags(s):
                at = place(tag)
                self.to_y(self.buf.at[at, y], at, tag)

        def across(self, s):
            for tag in tags(s):
                at = place(tag)
                rightward = tag[0] == 0 and tag[1] < 8
                self.yl[tag].wait_recv()
                if rightward:
                    self.yo[tag] = send(self.buf.at[at, yl], self.buf.at[at, yl], dev_yr)
                self.yr[tag].wait_recv()
                if not rightward:
                    self.yo[tag] = send(self.buf.at[at, yr], self.buf.at[at, yr], dev_yl)

        def done(self, s):
            for tag in tags(s):
                self.yo[tag].wait_recv()

    class YFirst:
        def __init__(self, own, buf):
            self.own, self.buf = own, buf
            self.left, self.right = {}, {}

        def begin_piece(self, p, col, src):
            self.left[p, 0] = send(src, self.buf.at[z, col], dev_zr)
            self.right[p, 0] = send(src, self.buf.at[z, col], dev_zl)

        def start(self):
            self.from_l = send(self.own, self.buf.at[z, y], dev_yr)
            self.from_r = send(self.own, self.buf.at[z, y], dev_yl)
            self.begin_piece(0, y, self.own)

        def begin(self):
            self.from_l.wait_recv()
            block = self.buf.at[z, yl]
            self.from_o = send(block, block, dev_yr)
            self.begin_piece(1, yl, block)
            self.from_r.wait_recv()
            self.begin_piece(2, yr, self.buf.at[z, yr])

        def begin_last(self):
            self.from_o.wait_recv()
            self.begin_piece(3, yo, self.buf.at[z, yo])

        def ring(self, s):
            for p, col in enumerate((y, yl, yr, yo)):
                self.left[p, s - 1].wait_recv()
                if s < 8:
                    block = self.buf.at[zm(s), col]
                    self.left[p, s] = send(block, block, dev_zr)
                if s <= 7:
                    self.right[p, s - 1].wait_recv()
                    if s < 7:
                        block = self.buf.at[zp(s), col]
                        self.right[p, s] = send(block, block, dev_zl)

    def x_start(src, slot):
        own = slot(x, c)
        return {"l": send(src, own, dev_xr), "r": send(src, own, dev_xl), "p": send(src, own, dev_p)}

    def x_forward(g, slot, halves):
        left, right = slot(xl, c), slot(xr, c)
        g["l"].wait_recv()
        g["a"] = send(halves(left)[0], halves(left)[0], dev_xr)
        g["pl"] = send(left, left, dev_p)
        g["r"].wait_recv()
        g["b"] = send(halves(right)[1], halves(right)[1], dev_xl)
        g["pr"] = send(right, right, dev_p)

    def x_relay(g, slot, halves):
        a, b = halves(slot(xo, c))
        g["a"].wait_recv()
        g["pa"] = send(a, a, dev_p)
        g["b"].wait_recv()
        g["pb"] = send(b, b, dev_p)

    def x_done(g):
        for name in ("p", "pl", "pr", "pa", "pb"):
            g[name].wait_recv()

    def ow_slot(a, b):
        return ow.at[a * NC + b]

    def ow_halves(ref):
        return ref.at[pl.ds(0, 64)], ref.at[pl.ds(64, 64)]

    def att_slot(a, b):
        return att.at[a * NC + b]

    def att_halves(ref):
        return ref.at[pl.ds(0, 192)], ref.at[pl.ds(192, 192)]

    def out_slot(a, b):
        return out.at[b * NX + a]

    def lane_halves(ref):
        return ref.at[:, pl.ds(0, D // 2)], ref.at[:, pl.ds(D // 2, D // 2)]

    ga = ZFirst(gate_w.at[:, pl.ds(0, MAIN)], wga)
    gb = YFirst(gb_own, wgb)
    dn = ZFirst(dn_own, wd)
    halo = [
        send(key.at[pl.ds(256, 128), lanes], kext.at[pl.ds(0, 128)], dev_after),
        send(value.at[pl.ds(256, 128), lanes], vext.at[pl.ds(0, 128)], dev_after),
        send(dsend.at[0], dext.at[0], dev_after),
        send(key.at[pl.ds(0, 128), lanes], kext.at[pl.ds(512, 128)], dev_before),
        send(value.at[pl.ds(0, 128), lanes], vext.at[pl.ds(512, 128)], dev_before),
        send(dsend.at[1], dext.at[1], dev_before),
    ]
    gb.start()
    ga.start()
    ow_g = x_start(out_w, ow_slot)
    ow[x * NC + c] = out_w[...]
    gb.begin()

    def attend(block):
        q = query[pl.ds(block * 128, 128), :]
        k = kext[pl.ds(block * 128, 384), :]
        v = vext[pl.ds(block * 128, 384), :]
        scores = lax.dot_general(q, k, (((1,), (1,)), ((), ())), preferred_element_type=F32)
        scores = scores * HD ** (-0.5)
        if block == 0:
            first = jnp.where(sp == 0, -1, dext[0, 0:1])
        else:
            first = docs[block - 1 : block]
        if block == 2:
            last = jnp.where(sp == NZ * NY - 1, -1, dext[1, 0:1])
        else:
            last = docs[block + 1 : block + 2]
        around = jnp.concatenate([first, docs[block : block + 1], last], axis=1)
        mine = jnp.transpose(jnp.broadcast_to(docs[block : block + 1], (128, 128)))[:, 0:1]
        row = lax.broadcasted_iota(jnp.int32, (128, 384), 0)
        col = lax.broadcasted_iota(jnp.int32, (128, 384), 1)
        allowed = (col >= row) & (col <= row + 2 * WIN) & (mine == around)
        masked = jnp.where(allowed, scores, LOW)
        here = sink[0]
        peak = jnp.maximum(jnp.max(masked, axis=1, keepdims=True), here)
        lifted = jnp.where(allowed, jnp.exp(masked - peak), 0.0)
        denom = jnp.sum(lifted, axis=1, keepdims=True) + jnp.exp(here - peak)
        probs = (lifted / denom).astype(BF)
        attended = jnp.dot(probs, v, preferred_element_type=F32).astype(BF)
        att[x * NC + c, pl.ds(block * 128, 128), :] = attended

    attend(1)
    gb.begin_last()
    for copy in halo:
        copy.wait_recv()
    attend(0)
    ga.ring(1)
    gb.ring(1)
    attend(2)
    ga.across(0)
    ga.ring(2)
    gb.ring(2)
    att_g = x_start(att.at[x * NC + c], att_slot)
    ga.across(1)
    dn.start()
    x_forward(ow_g, ow_slot, ow_halves)
    ga.ring(3)
    gb.ring(3)
    x_forward(att_g, att_slot, att_halves)
    ga.across(2)
    dn.ring(1)
    ga.ring(4)
    gb.ring(4)
    x_relay(ow_g, ow_slot, ow_halves)
    x_relay(att_g, att_slot, att_halves)
    ga.across(3)
    dn.across(0)
    dn.ring(2)
    x_done(ow_g)
    x_done(att_g)
    stream_copy.wait()

    def project(n, squares):
        cols = pl.ds(pl.multiple_of(n * 256, 256), 256)
        left = jnp.concatenate([att[h] for h in range(8)], axis=1)
        right = ow[:, :, cols].reshape(1024, 256)
        branch = jnp.dot(left, right, preferred_element_type=F32).astype(BF)
        total = (stream[:, cols].astype(F32) + branch.astype(F32)).astype(BF)
        carried[:, :, cols] = total.reshape(8, OWN, 256)
        wide = total.astype(F32)
        return squares + jnp.sum(wide * wide, axis=1, keepdims=True)

    squares = lax.fori_loop(0, 8, project, jnp.zeros((TOK, 1), F32))
    scale = lax.rsqrt(squares / D + EPS)

    ga.ring(5)
    gb.ring(5)

    def normalize(n, carry):
        cols = pl.ds(pl.multiple_of(n * 256, 256), 256)
        wide = carried[:, :, cols].reshape(TOK, 256).astype(F32)
        normed[:, cols] = (wide * scale * gain[:, cols]).astype(BF)
        return carry

    lax.fori_loop(0, 8, normalize, 0)
    ga.across(4)
    dn.across(1)
    dn.ring(3)

    def accumulate(za, zb, first):
        left = jnp.concatenate(
            [
                normed[:, pl.ds(pl.multiple_of(za * 128, 128), 128)],
                normed[:, pl.ds(pl.multiple_of(zb * 128, 128), 128)],
            ],
            axis=1,
        )
        for buf, acc, width in ((wga, acc_a, MAIN), (wgb, acc_b, FP)):
            right = jnp.concatenate([buf[za].reshape(128, width), buf[zb].reshape(128, width)], axis=0)
            term = jnp.dot(left, right, preferred_element_type=F32)
            if first:
                acc[...] = term
            else:
                acc[...] += term

    def accumulate_tag(s, first=False):
        accumulate(zm(s), zp(s), first)

    ga.done(1)
    accumulate_tag(1, True)
    ga.ring(6)
    gb.ring(6)
    ga.across(5)
    dn.across(2)
    dn.ring(4)
    ga.done(2)
    ga.done(3)

    def both(i, carry):
        accumulate_tag(i)
        return carry

    lax.fori_loop(2, 4, both, 0)
    ga.ring(7)
    gb.ring(7)
    ga.across(6)
    dn.across(3)
    dn.ring(5)
    ga.done(4)
    accumulate_tag(4)
    ga.ring(8)
    gb.ring(8)
    ga.across(7)
    dn.across(4)
    dn.ring(6)
    ga.done(5)
    accumulate_tag(5)
    ga.across(8)
    dn.across(5)
    dn.ring(7)
    ga.done(6)
    accumulate_tag(6)
    ga.done(7)
    accumulate_tag(7)
    dn.across(6)
    dn.ring(8)
    ga.done(0)
    ga.done(8)
    accumulate(z, zm(8), False)
    dn.across(7)

    gate, up = acc_a[...], acc_b[:, 0:MAIN]
    hid[:, 0:MAIN] = (gate / (1.0 + jnp.exp(-gate)) * up).astype(BF)
    rest = acc_b[:, MAIN:FP]
    swapped = pltpu.roll(rest, TAIL, 1)
    tail = rest / (1.0 + jnp.exp(-rest)) * swapped
    lane = lax.broadcasted_iota(jnp.int32, (TOK, 2 * TAIL), 1)
    hid[:, MAIN:FP] = jnp.where(lane < TAIL, tail, 0.0).astype(BF)
    dn.across(8)
    for s in range(9):
        dn.done(s)

    def lower(n, carry):
        w = wd[pl.ds(2 * n, 2)].reshape(256, FP)
        term = lax.dot_general(hid[...], w, (((1,), (1,)), ((), ())), preferred_element_type=F32)
        cols = pl.ds(pl.multiple_of(n * 256, 256), 256)
        part[:, :, :, cols] = term.astype(BF).reshape(NC, NX, OWN, 256)
        return carry

    lax.fori_loop(0, 8, lower, 0)

    to_pair = send(part.at[pc], pair_in, dev_p)
    to_pair.wait_recv()

    def fold(i, carry):
        at = lax.rem(xo + i, NX)
        summed[at] = (part[c, at].astype(F32) + pair_in[at].astype(F32)).astype(BF)
        return carry

    lax.fori_loop(0, 4, fold, 0)
    half = D // 2
    low, high = pl.ds(0, half), pl.ds(half, half)
    opp_a = send(summed.at[xo, :, low], opp_in.at[0], dev_xr)
    opp_b = send(summed.at[xo, :, high], opp_in.at[1], dev_xl)
    near_b = send(summed.at[xr, :, high], near_in.at[1], dev_xr)
    near_a = send(summed.at[xl, :, low], near_in.at[0], dev_xl)
    opp_a.wait_recv()
    relay[0] = (opp_in[0].astype(F32) + summed[xr, :, low].astype(F32)).astype(BF)
    opp_b.wait_recv()
    relay[1] = (opp_in[1].astype(F32) + summed[xl, :, high].astype(F32)).astype(BF)
    far_a = send(relay.at[0], far_in.at[0], dev_xr)
    far_b = send(relay.at[1], far_in.at[1], dev_xl)
    near_a.wait_recv()
    near_b.wait_recv()
    own = c * NX + x
    for i, arrived in ((0, far_a), (1, far_b)):
        arrived.wait_recv()
        cols = pl.ds(i * half, half)
        feed = summed[x, :, cols].astype(F32) + near_in[i].astype(F32) + far_in[i].astype(F32)
        feed = feed.astype(BF).astype(F32)
        out[own, :, cols] = (carried[own, :, cols].astype(F32) + 0.5 * feed).astype(BF)
    out_g = x_start(out.at[own], out_slot)
    x_forward(out_g, out_slot, lane_halves)
    x_relay(out_g, out_slot, lane_halves)
    x_done(out_g)
    for copy in started:
        copy.wait_send()


def per_device(
    stream,
    query_rows,
    key_rows,
    value_rows,
    doc_ids,
    sink_logit,
    out_weight,
    norm_gain,
    gate_weight,
    up_weight,
    down_weight,
):
    vmem = pl.BlockSpec(memory_space=pltpu.VMEM)
    smem = pl.BlockSpec(memory_space=pltpu.SMEM)
    far = pl.BlockSpec(memory_space=pl.ANY)
    result = pl.pallas_call(
        kernel,
        name="layer",
        out_shape=jax.ShapeDtypeStruct((8, OWN, D), BF),
        in_specs=[far] + [vmem] * 4 + [smem] + [vmem] * 5,
        out_specs=vmem,
        scratch_shapes=[
            pltpu.VMEM((TOK, D), BF),
            pltpu.VMEM((TOK + 2 * WIN, HD), BF),
            pltpu.VMEM((TOK + 2 * WIN, HD), BF),
            pltpu.VMEM((2, 8, 128), jnp.int32),
            pltpu.VMEM((2, 8, 128), jnp.int32),
            pltpu.VMEM((32, FP), BF),
            pltpu.VMEM((32, FP), BF),
            pltpu.VMEM((NZ, NY, 32, MAIN), BF),
            pltpu.VMEM((NZ, NY, 32, FP), BF),
            pltpu.VMEM((NZ, NY, 32, FP), BF),
            pltpu.VMEM((8, 128, D), BF),
            pltpu.VMEM((8, TOK, HD), BF),
            pltpu.VMEM((8, OWN, D), BF),
            pltpu.VMEM((TOK, D), BF),
            pltpu.VMEM((TOK, MAIN), F32),
            pltpu.VMEM((TOK, FP), F32),
            pltpu.VMEM((TOK, FP), BF),
            pltpu.VMEM((NC, NX, OWN, D), BF),
            pltpu.VMEM((NX, OWN, D), BF),
            pltpu.VMEM((NX, OWN, D), BF),
            pltpu.VMEM((2, OWN, D // 2), BF),
            pltpu.VMEM((2, OWN, D // 2), BF),
            pltpu.VMEM((2, OWN, D // 2), BF),
            pltpu.VMEM((2, OWN, D // 2), BF),
            pltpu.SemaphoreType.DMA,
            pltpu.SemaphoreType.DMA((COPIES,)),
            pltpu.SemaphoreType.DMA((COPIES,)),
        ],
        compiler_params=pltpu.CompilerParams(
            collective_id=0, has_side_effects=True, vmem_limit_bytes=60 * 1024 * 1024
        ),
    )(
        stream,
        query_rows,
        key_rows,
        value_rows,
        doc_ids.reshape(3, 128),
        sink_logit,
        out_weight,
        norm_gain.reshape(1, D),
        gate_weight,
        up_weight,
        down_weight.T,
    )
    return result.reshape(TOK, D)


def solution(mesh):
    split = Mesh(mesh.devices.reshape(NZ, NY, NX, NC), ("z", "y", "x", "c"))
    placed = (
        P(SP, None),
        P(SP, TP),
        P(SP, None),
        P(SP, None),
        P(SP),
        P(TP),
        P(TP, None),
        P(),
        P(SP, TP),
        P(SP, TP),
        P(TP, SP),
    )
    return jax.shard_map(
        per_device, mesh=split, in_specs=placed, out_specs=P(SP, None), check_vma=False
    )
```

```python
import jax
import jax.numpy as jnp
from jax import lax
from jax.experimental import pallas as pl
from jax.experimental.pallas import tpu as pltpu
from jax.sharding import Mesh
from jax.sharding import PartitionSpec as P

HD = 128
WIN = 128
NZ, NY, NX, NC = 16, 4, 4, 2
TOK = 384
D = 2048
FFL = 704
MAIN = 640
TAIL = 64
FP = 768
OWN = TOK // (NX * NC)
EPS = 1e-06
LOW = -1e30
COPIES = 280
CHUNK = D // 4
HALF = CHUNK // 2
SP = ("z", "y")
TP = ("x", "c")
F32 = jnp.float32
BF = jnp.bfloat16


def kernel(
    stream_far,
    query,
    key,
    value,
    docs,
    sink,
    out_w,
    gain,
    gate_w,
    up_w,
    down_w,
    out,
    stream,
    kext,
    vext,
    dsend,
    dext,
    gb_own,
    dn_own,
    wga,
    wgb,
    wd,
    ow,
    att,
    carried,
    normed,
    acc_a,
    acc_b,
    hid,
    part,
    summed,
    pair_in,
    opp_in,
    relay,
    near_in,
    far_in,
    shuffled,
    local_sem,
    out_sems,
    send_sems,
    recv_sems,
):
    z, y = lax.axis_index("z"), lax.axis_index("y")
    x, c = lax.axis_index("x"), lax.axis_index("c")
    zr, zl = lax.rem(z + 1, NZ), lax.rem(z + NZ - 1, NZ)
    yr, yl = lax.rem(y + 1, NY), lax.rem(y + NY - 1, NY)
    xr, xl = lax.rem(x + 1, NX), lax.rem(x + NX - 1, NX)
    yo, xo = lax.rem(y + 2, NY), lax.rem(x + 2, NX)
    pc = 1 - c
    sp = z * NY + y
    after, before = lax.rem(sp + 1, NZ * NY), lax.rem(sp + NZ * NY - 1, NZ * NY)
    dev_zr, dev_zl = (zr, y, x, c), (zl, y, x, c)
    dev_yr, dev_yl = (z, yr, x, c), (z, yl, x, c)
    dev_xr, dev_xl = (z, y, xr, c), (z, y, xl, c)
    dev_p = (z, y, x, pc)
    dev_after = (after // NY, lax.rem(after, NY), x, c)
    dev_before = (before // NY, lax.rem(before, NY), x, c)

    barrier = pltpu.get_barrier_semaphore()
    peers = (dev_zr, dev_zl, dev_yr, dev_yl, dev_xr, dev_xl, dev_p, dev_after, dev_before)
    for peer in peers:
        pl.semaphore_signal(barrier, inc=1, device_id=peer, device_id_type=pl.DeviceIdType.MESH)
    stream_copy = pltpu.make_async_copy(stream_far, stream, local_sem)
    stream_copy.start()

    gb_own[:, 0:MAIN] = up_w[:, 0:MAIN]
    gb_own[:, MAIN:FP] = jnp.concatenate([gate_w[:, MAIN:FFL], up_w[:, MAIN:FFL]], axis=1)
    dn_own[:, 0:MAIN] = down_w[:, 0:MAIN]
    dn_own[:, MAIN:FP] = jnp.concatenate([down_w[:, MAIN:FFL], jnp.zeros((32, TAIL), BF)], axis=1)
    dsend[0] = jnp.broadcast_to(docs[2:3], (8, 128))
    dsend[1] = jnp.broadcast_to(docs[0:1], (8, 128))
    group = pl.multiple_of((x // 2) * HD, HD)
    lanes = pl.ds(group, HD)
    kext[pl.ds(128, 384), :] = key[:, lanes]
    vext[pl.ds(128, 384), :] = value[:, lanes]
    wga[z, y] = gate_w[:, 0:MAIN]
    wgb[z, y] = gb_own[...]
    wd[z, y] = dn_own[...]

    pl.semaphore_wait(barrier, len(peers))

    started = []

    def send(src, dst, dev):
        at = len(started)
        copy = pltpu.make_async_remote_copy(
            src_ref=src,
            dst_ref=dst,
            send_sem=send_sems.at[at],
            recv_sem=recv_sems.at[at],
            device_id=dev,
            device_id_type=pl.DeviceIdType.MESH,
        )
        copy.start()
        started.append(copy)
        return copy

    def zm(s):
        return lax.rem(z + NZ - s, NZ)

    def zp(s):
        return lax.rem(z + s, NZ)

    def tags(s):
        if s == 0:
            return [(0, 0)]
        if s == 8:
            return [(0, 8)]
        return [(0, s), (1, s)]

    def place(tag):
        return zm(tag[1]) if tag[0] == 0 else zp(tag[1])

    class ZFirst:
        def __init__(self, own, buf):
            self.own, self.buf = own, buf
            self.left, self.right, self.yl, self.yr, self.yo = {}, {}, {}, {}, {}

        def to_y(self, src, at, tag):
            self.yl[tag] = send(src, self.buf.at[at, y], dev_yr)
            self.yr[tag] = send(src, self.buf.at[at, y], dev_yl)

        def start(self):
            self.left[0] = send(self.own, self.buf.at[z, y], dev_zr)
            self.right[0] = send(self.own, self.buf.at[z, y], dev_zl)
            self.to_y(self.own, z, (0, 0))

        def ring(self, s):
            block = self.buf.at[zm(s), y]
            self.left[s - 1].wait_recv()
            if s < 8:
                self.left[s] = send(block, block, dev_zr)
            if s <= 7:
                block = self.buf.at[zp(s), y]
                self.right[s - 1].wait_recv()
                if s < 7:
                    self.right[s] = send(block, block, dev_zl)
            for tag in tags(s):
                at = place(tag)
                self.to_y(self.buf.at[at, y], at, tag)

        def across(self, s):
            for tag in tags(s):
                at = place(tag)
                rightward = tag[0] == 0 and tag[1] < 8
                self.yl[tag].wait_recv()
                if rightward:
                    self.yo[tag] = send(self.buf.at[at, yl], self.buf.at[at, yl], dev_yr)
                self.yr[tag].wait_recv()
                if not rightward:
                    self.yo[tag] = send(self.buf.at[at, yr], self.buf.at[at, yr], dev_yl)

        def done(self, s):
            for tag in tags(s):
                self.yo[tag].wait_recv()

    class YFirst:
        def __init__(self, own, buf):
            self.own, self.buf = own, buf
            self.left, self.right = {}, {}

        def begin_piece(self, p, col, src):
            self.left[p, 0] = send(src, self.buf.at[z, col], dev_zr)
            self.right[p, 0] = send(src, self.buf.at[z, col], dev_zl)

        def start(self):
            self.from_l = send(self.own, self.buf.at[z, y], dev_yr)
            self.from_r = send(self.own, self.buf.at[z, y], dev_yl)
            self.begin_piece(0, y, self.own)

        def begin(self):
            self.from_l.wait_recv()
            block = self.buf.at[z, yl]
            self.from_o = send(block, block, dev_yr)
            self.begin_piece(1, yl, block)
            self.from_r.wait_recv()
            self.begin_piece(2, yr, self.buf.at[z, yr])

        def begin_last(self):
            self.from_o.wait_recv()
            self.begin_piece(3, yo, self.buf.at[z, yo])

        def ring(self, s):
            for p, col in enumerate((y, yl, yr, yo)):
                self.left[p, s - 1].wait_recv()
                if s < 8:
                    block = self.buf.at[zm(s), col]
                    self.left[p, s] = send(block, block, dev_zr)
                if s <= 7:
                    self.right[p, s - 1].wait_recv()
                    if s < 7:
                        block = self.buf.at[zp(s), col]
                        self.right[p, s] = send(block, block, dev_zl)

    def x_start(src, slot):
        own = slot(x, c)
        return {"l": send(src, own, dev_xr), "r": send(src, own, dev_xl), "p": send(src, own, dev_p)}

    def x_forward(g, slot, halves):
        left, right = slot(xl, c), slot(xr, c)
        g["l"].wait_recv()
        g["a"] = send(halves(left)[0], halves(left)[0], dev_xr)
        g["pl"] = send(left, left, dev_p)
        g["r"].wait_recv()
        g["b"] = send(halves(right)[1], halves(right)[1], dev_xl)
        g["pr"] = send(right, right, dev_p)

    def x_relay(g, slot, halves):
        a, b = halves(slot(xo, c))
        g["a"].wait_recv()
        g["pa"] = send(a, a, dev_p)
        g["b"].wait_recv()
        g["pb"] = send(b, b, dev_p)

    def x_done(g):
        for name in ("p", "pl", "pr", "pa", "pb"):
            g[name].wait_recv()

    def ow_slot(a, b):
        return ow.at[a * NC + b]

    def ow_halves(ref):
        return ref.at[pl.ds(0, 64)], ref.at[pl.ds(64, 64)]

    def att_slot(a, b):
        return att.at[a * NC + b]

    def att_halves(ref):
        return ref.at[pl.ds(0, 192)], ref.at[pl.ds(192, 192)]

    def lane_halves(ref):
        return ref.at[:, pl.ds(0, HALF)], ref.at[:, pl.ds(HALF, HALF)]

    ga = ZFirst(gate_w.at[:, pl.ds(0, MAIN)], wga)
    gb = YFirst(gb_own, wgb)
    dn = ZFirst(dn_own, wd)
    halo = [
        send(key.at[pl.ds(256, 128), lanes], kext.at[pl.ds(0, 128)], dev_after),
        send(value.at[pl.ds(256, 128), lanes], vext.at[pl.ds(0, 128)], dev_after),
        send(dsend.at[0], dext.at[0], dev_after),
        send(key.at[pl.ds(0, 128), lanes], kext.at[pl.ds(512, 128)], dev_before),
        send(value.at[pl.ds(0, 128), lanes], vext.at[pl.ds(512, 128)], dev_before),
        send(dsend.at[1], dext.at[1], dev_before),
    ]
    gb.start()
    ga.start()
    ow_g = x_start(out_w, ow_slot)
    ow[x * NC + c] = out_w[...]
    gb.begin()

    def attend(block):
        q = query[pl.ds(block * 128, 128), :]
        k = kext[pl.ds(block * 128, 384), :]
        v = vext[pl.ds(block * 128, 384), :]
        scores = lax.dot_general(q, k, (((1,), (1,)), ((), ())), preferred_element_type=F32)
        scores = scores * HD ** (-0.5)
        if block == 0:
            first = jnp.where(sp == 0, -1, dext[0, 0:1])
        else:
            first = docs[block - 1 : block]
        if block == 2:
            last = jnp.where(sp == NZ * NY - 1, -1, dext[1, 0:1])
        else:
            last = docs[block + 1 : block + 2]
        around = jnp.concatenate([first, docs[block : block + 1], last], axis=1)
        mine = jnp.transpose(jnp.broadcast_to(docs[block : block + 1], (128, 128)))[:, 0:1]
        row = lax.broadcasted_iota(jnp.int32, (128, 384), 0)
        col = lax.broadcasted_iota(jnp.int32, (128, 384), 1)
        allowed = (col >= row) & (col <= row + 2 * WIN) & (mine == around)
        masked = jnp.where(allowed, scores, LOW)
        here = sink[0]
        peak = jnp.maximum(jnp.max(masked, axis=1, keepdims=True), here)
        lifted = jnp.where(allowed, jnp.exp(masked - peak), 0.0)
        denom = jnp.sum(lifted, axis=1, keepdims=True) + jnp.exp(here - peak)
        probs = (lifted / denom).astype(BF)
        attended = jnp.dot(probs, v, preferred_element_type=F32).astype(BF)
        att[x * NC + c, pl.ds(block * 128, 128), :] = attended

    attend(1)
    gb.begin_last()
    for copy in halo:
        copy.wait_recv()
    attend(0)
    ga.ring(1)
    gb.ring(1)
    attend(2)
    ga.across(0)
    ga.ring(2)
    gb.ring(2)
    att_g = x_start(att.at[x * NC + c], att_slot)
    ga.across(1)
    dn.start()
    x_forward(ow_g, ow_slot, ow_halves)
    ga.ring(3)
    gb.ring(3)
    x_forward(att_g, att_slot, att_halves)
    ga.across(2)
    dn.ring(1)
    ga.ring(4)
    gb.ring(4)
    x_relay(ow_g, ow_slot, ow_halves)
    x_relay(att_g, att_slot, att_halves)
    ga.across(3)
    dn.across(0)
    dn.ring(2)
    x_done(ow_g)
    x_done(att_g)
    stream_copy.wait()

    def project(n, squares):
        cols = pl.ds(pl.multiple_of(n * 256, 256), 256)
        left = jnp.concatenate([att[h] for h in range(8)], axis=1)
        right = ow[:, :, cols].reshape(1024, 256)
        branch = jnp.dot(left, right, preferred_element_type=F32).astype(BF)
        total = (stream[:, cols].astype(F32) + branch.astype(F32)).astype(BF)
        carried[:, :, cols] = total.reshape(8, OWN, 256)
        wide = total.astype(F32)
        return squares + jnp.sum(wide * wide, axis=1, keepdims=True)

    squares = lax.fori_loop(0, 8, project, jnp.zeros((TOK, 1), F32))
    scale = lax.rsqrt(squares / D + EPS)

    ga.ring(5)
    gb.ring(5)

    def normalize(n, carry):
        cols = pl.ds(pl.multiple_of(n * 256, 256), 256)
        wide = carried[:, :, cols].reshape(TOK, 256).astype(F32)
        normed[:, cols] = (wide * scale * gain[:, cols]).astype(BF)
        return carry

    lax.fori_loop(0, 8, normalize, 0)
    ga.across(4)
    dn.across(1)
    dn.ring(3)

    def accumulate(za, zb, first):
        left = jnp.concatenate(
            [
                normed[:, pl.ds(pl.multiple_of(za * 128, 128), 128)],
                normed[:, pl.ds(pl.multiple_of(zb * 128, 128), 128)],
            ],
            axis=1,
        )
        for buf, acc, width in ((wga, acc_a, MAIN), (wgb, acc_b, FP)):
            right = jnp.concatenate([buf[za].reshape(128, width), buf[zb].reshape(128, width)], axis=0)
            term = jnp.dot(left, right, preferred_element_type=F32)
            if first:
                acc[...] = term
            else:
                acc[...] += term

    def accumulate_tag(s, first=False):
        accumulate(zm(s), zp(s), first)

    ga.done(1)
    accumulate_tag(1, True)
    ga.ring(6)
    gb.ring(6)
    ga.across(5)
    dn.across(2)
    dn.ring(4)
    ga.done(2)
    ga.done(3)

    def both(i, carry):
        accumulate_tag(i)
        return carry

    lax.fori_loop(2, 4, both, 0)
    ga.ring(7)
    gb.ring(7)
    ga.across(6)
    dn.across(3)
    dn.ring(5)
    ga.done(4)
    accumulate_tag(4)
    ga.ring(8)
    gb.ring(8)
    ga.across(7)
    dn.across(4)
    dn.ring(6)
    ga.done(5)
    accumulate_tag(5)
    ga.across(8)
    dn.across(5)
    dn.ring(7)
    ga.done(6)
    accumulate_tag(6)
    ga.done(7)
    accumulate_tag(7)
    dn.across(6)
    dn.ring(8)
    ga.done(0)
    ga.done(8)
    accumulate(z, zm(8), False)
    dn.across(7)

    gate, up = acc_a[...], acc_b[:, 0:MAIN]
    hid[:, 0:MAIN] = (gate / (1.0 + jnp.exp(-gate)) * up).astype(BF)
    rest = acc_b[:, MAIN:FP]
    swapped = pltpu.roll(rest, TAIL, 1)
    tail = rest / (1.0 + jnp.exp(-rest)) * swapped
    lane = lax.broadcasted_iota(jnp.int32, (TOK, 2 * TAIL), 1)
    hid[:, MAIN:FP] = jnp.where(lane < TAIL, tail, 0.0).astype(BF)

    own = c * NX + x
    low, high = pl.ds(0, HALF), pl.ds(HALF, HALF)
    chunks = [{} for _ in range(4)]
    written = []

    def groups(k):
        if k == 3:
            return [zm(7), zp(7), z, zm(8)]
        return [zm(2 * k + 1), zp(2 * k + 1), zm(2 * k + 2), zp(2 * k + 2)]

    def lower(k):
        at = groups(k)
        for i in (0, 2):
            w = jnp.concatenate([wd[at[i]].reshape(128, FP), wd[at[i + 1]].reshape(128, FP)], axis=0)
            term = lax.dot_general(hid[...], w, (((1,), (1,)), ((), ())), preferred_element_type=F32)
            part[k, :, :, :, pl.ds(i * 128, 256)] = term.astype(BF).reshape(NC, NX, OWN, 256)
        chunks[k]["pair"] = send(part.at[k, pc], pair_in.at[k], dev_p)

    def fold(k):
        g = chunks[k]
        g["pair"].wait_recv()
        summed[k] = (part[k, c].astype(F32) + pair_in[k].astype(F32)).astype(BF)
        g["opp_a"] = send(summed.at[k, xo, :, low], opp_in.at[k, 0], dev_xr)
        g["opp_b"] = send(summed.at[k, xo, :, high], opp_in.at[k, 1], dev_xl)
        g["near_b"] = send(summed.at[k, xr, :, high], near_in.at[k, 1], dev_xr)
        g["near_a"] = send(summed.at[k, xl, :, low], near_in.at[k, 0], dev_xl)

    def pass_on(k):
        g = chunks[k]
        g["opp_a"].wait_recv()
        relay[k, 0] = (opp_in[k, 0].astype(F32) + summed[k, xr, :, low].astype(F32)).astype(BF)
        g["far_a"] = send(relay.at[k, 0], far_in.at[k, 0], dev_xr)
        g["opp_b"].wait_recv()
        relay[k, 1] = (opp_in[k, 1].astype(F32) + summed[k, xl, :, high].astype(F32)).astype(BF)
        g["far_b"] = send(relay.at[k, 1], far_in.at[k, 1], dev_xl)

    def slot(k):
        return lambda a, b: shuffled.at[k, b * NX + a]

    def mix(k):
        g = chunks[k]
        base = jnp.concatenate(
            [carried[own, :, pl.ds(pl.multiple_of(at * 128, 128), 128)] for at in groups(k)], axis=1
        ).astype(F32)
        g["near_a"].wait_recv()
        g["near_b"].wait_recv()
        for i, name in ((0, "far_a"), (1, "far_b")):
            g[name].wait_recv()
            cols = pl.ds(i * HALF, HALF)
            feed = summed[k, x, :, cols].astype(F32) + near_in[k, i].astype(F32) + far_in[k, i].astype(F32)
            feed = feed.astype(BF).astype(F32)
            shuffled[k, own, :, cols] = (base[:, i * HALF : (i + 1) * HALF] + 0.5 * feed).astype(BF)
        g["out"] = x_start(shuffled.at[k, own], slot(k))

    def forward(k):
        x_forward(chunks[k]["out"], slot(k), lane_halves)

    def hand_over(k):
        x_relay(chunks[k]["out"], slot(k), lane_halves)

    def write(k):
        x_done(chunks[k]["out"])
        for i, at in enumerate(groups(k)):
            copy = pltpu.make_async_copy(
                shuffled.at[k, :, :, pl.ds(i * 128, 128)],
                out.at[:, :, pl.ds(pl.multiple_of(at * 128, 128), 128)],
                out_sems.at[len(written)],
            )
            copy.start()
            written.append(copy)

    dn.done(1)
    dn.done(2)
    lower(0)
    dn.across(8)
    dn.done(3)
    dn.done(4)
    lower(1)
    fold(0)
    dn.done(5)
    dn.done(6)
    lower(2)
    pass_on(0)
    fold(1)
    dn.done(7)
    dn.done(0)
    dn.done(8)
    lower(3)
    pass_on(1)
    fold(2)
    mix(0)
    fold(3)
    pass_on(2)
    mix(1)
    pass_on(3)
    forward(0)
    mix(2)
    forward(1)
    hand_over(0)
    mix(3)
    forward(2)
    hand_over(1)
    write(0)
    forward(3)
    hand_over(2)
    write(1)
    hand_over(3)
    write(2)
    write(3)
    for copy in written:
        copy.wait()
    for copy in started:
        copy.wait_send()


def per_device(
    stream,
    query_rows,
    key_rows,
    value_rows,
    doc_ids,
    sink_logit,
    out_weight,
    norm_gain,
    gate_weight,
    up_weight,
    down_weight,
):
    vmem = pl.BlockSpec(memory_space=pltpu.VMEM)
    smem = pl.BlockSpec(memory_space=pltpu.SMEM)
    far = pl.BlockSpec(memory_space=pl.ANY)
    result = pl.pallas_call(
        kernel,
        name="layer",
        out_shape=jax.ShapeDtypeStruct((8, OWN, D), BF),
        in_specs=[far] + [vmem] * 4 + [smem] + [vmem] * 5,
        out_specs=far,
        scratch_shapes=[
            pltpu.VMEM((TOK, D), BF),
            pltpu.VMEM((TOK + 2 * WIN, HD), BF),
            pltpu.VMEM((TOK + 2 * WIN, HD), BF),
            pltpu.VMEM((2, 8, 128), jnp.int32),
            pltpu.VMEM((2, 8, 128), jnp.int32),
            pltpu.VMEM((32, FP), BF),
            pltpu.VMEM((32, FP), BF),
            pltpu.VMEM((NZ, NY, 32, MAIN), BF),
            pltpu.VMEM((NZ, NY, 32, FP), BF),
            pltpu.VMEM((NZ, NY, 32, FP), BF),
            pltpu.VMEM((8, 128, D), BF),
            pltpu.VMEM((8, TOK, HD), BF),
            pltpu.VMEM((8, OWN, D), BF),
            pltpu.VMEM((TOK, D), BF),
            pltpu.VMEM((TOK, MAIN), F32),
            pltpu.VMEM((TOK, FP), F32),
            pltpu.VMEM((TOK, FP), BF),
            pltpu.VMEM((4, NC, NX, OWN, CHUNK), BF),
            pltpu.VMEM((4, NX, OWN, CHUNK), BF),
            pltpu.VMEM((4, NX, OWN, CHUNK), BF),
            pltpu.VMEM((4, 2, OWN, HALF), BF),
            pltpu.VMEM((4, 2, OWN, HALF), BF),
            pltpu.VMEM((4, 2, OWN, HALF), BF),
            pltpu.VMEM((4, 2, OWN, HALF), BF),
            pltpu.VMEM((4, 8, OWN, CHUNK), BF),
            pltpu.SemaphoreType.DMA,
            pltpu.SemaphoreType.DMA((16,)),
            pltpu.SemaphoreType.DMA((COPIES,)),
            pltpu.SemaphoreType.DMA((COPIES,)),
        ],
        compiler_params=pltpu.CompilerParams(
            collective_id=0, has_side_effects=True, vmem_limit_bytes=60 * 1024 * 1024
        ),
    )(
        stream,
        query_rows,
        key_rows,
        value_rows,
        doc_ids.reshape(3, 128),
        sink_logit,
        out_weight,
        norm_gain.reshape(1, D),
        gate_weight,
        up_weight,
        down_weight.T,
    )
    return result.reshape(TOK, D)


def solution(mesh):
    split = Mesh(mesh.devices.reshape(NZ, NY, NX, NC), ("z", "y", "x", "c"))
    placed = (
        P(SP, None),
        P(SP, TP),
        P(SP, None),
        P(SP, None),
        P(SP),
        P(TP),
        P(TP, None),
        P(),
        P(SP, TP),
        P(SP, TP),
        P(TP, SP),
    )
    return jax.shard_map(
        per_device, mesh=split, in_specs=placed, out_specs=P(SP, None), check_vma=False
    )
```

```python
import jax
import jax.numpy as jnp
from jax import lax
from jax.experimental import pallas as pl
from jax.experimental.pallas import tpu as pltpu
from jax.sharding import Mesh
from jax.sharding import PartitionSpec as P

HD = 128
WIN = 128
NZ, NY, NX, NC = 16, 4, 4, 2
TOK = 384
D = 2048
FFL = 704
MAIN = 640
TAIL = 64
FP = 768
OWN = TOK // (NX * NC)
EPS = 1e-06
LOW = -1e30
COPIES = 280
CHUNK = D // 4
HALF = CHUNK // 2
SP = ("z", "y")
TP = ("x", "c")
F32 = jnp.float32
BF = jnp.bfloat16


def kernel(
    stream,
    query,
    key,
    value,
    docs,
    sink,
    out_w,
    gain,
    gate_w,
    up_w,
    down_w,
    out,
    kext,
    vext,
    dsend,
    dext,
    gb_own,
    dn_own,
    wga,
    wgb,
    wd,
    ow,
    att,
    carried,
    normed,
    acc_a,
    acc_b,
    hid,
    part,
    summed,
    pair_in,
    opp_in,
    relay,
    near_in,
    far_in,
    shuffled,
    send_sems,
    recv_sems,
):
    z, y = lax.axis_index("z"), lax.axis_index("y")
    x, c = lax.axis_index("x"), lax.axis_index("c")
    zr, zl = lax.rem(z + 1, NZ), lax.rem(z + NZ - 1, NZ)
    yr, yl = lax.rem(y + 1, NY), lax.rem(y + NY - 1, NY)
    xr, xl = lax.rem(x + 1, NX), lax.rem(x + NX - 1, NX)
    yo, xo = lax.rem(y + 2, NY), lax.rem(x + 2, NX)
    pc = 1 - c
    sp = z * NY + y
    after, before = lax.rem(sp + 1, NZ * NY), lax.rem(sp + NZ * NY - 1, NZ * NY)
    dev_zr, dev_zl = (zr, y, x, c), (zl, y, x, c)
    dev_yr, dev_yl = (z, yr, x, c), (z, yl, x, c)
    dev_xr, dev_xl = (z, y, xr, c), (z, y, xl, c)
    dev_p = (z, y, x, pc)
    dev_after = (after // NY, lax.rem(after, NY), x, c)
    dev_before = (before // NY, lax.rem(before, NY), x, c)

    barrier = pltpu.get_barrier_semaphore()
    peers = (dev_zr, dev_zl, dev_yr, dev_yl, dev_xr, dev_xl, dev_p, dev_after, dev_before)
    for peer in peers:
        pl.semaphore_signal(barrier, inc=1, device_id=peer, device_id_type=pl.DeviceIdType.MESH)

    gb_own[:, 0:MAIN] = up_w[:, 0:MAIN]
    gb_own[:, MAIN:FP] = jnp.concatenate([gate_w[:, MAIN:FFL], up_w[:, MAIN:FFL]], axis=1)
    dn_own[:, 0:MAIN] = down_w[:, 0:MAIN]
    dn_own[:, MAIN:FP] = jnp.concatenate([down_w[:, MAIN:FFL], jnp.zeros((32, TAIL), BF)], axis=1)
    dsend[0] = jnp.broadcast_to(docs[2:3], (8, 128))
    dsend[1] = jnp.broadcast_to(docs[0:1], (8, 128))
    group = pl.multiple_of((x // 2) * HD, HD)
    lanes = pl.ds(group, HD)
    kext[pl.ds(128, 384), :] = key[:, lanes]
    vext[pl.ds(128, 384), :] = value[:, lanes]
    wga[z, y] = gate_w[:, 0:MAIN]
    wgb[z, y] = gb_own[...]
    wd[z, y] = dn_own[...]

    pl.semaphore_wait(barrier, len(peers))

    started = []

    def send(src, dst, dev):
        at = len(started)
        copy = pltpu.make_async_remote_copy(
            src_ref=src,
            dst_ref=dst,
            send_sem=send_sems.at[at],
            recv_sem=recv_sems.at[at],
            device_id=dev,
            device_id_type=pl.DeviceIdType.MESH,
        )
        copy.start()
        started.append(copy)
        return copy

    def zm(s):
        return lax.rem(z + NZ - s, NZ)

    def zp(s):
        return lax.rem(z + s, NZ)

    def tags(s):
        if s == 0:
            return [(0, 0)]
        if s == 8:
            return [(0, 8)]
        return [(0, s), (1, s)]

    def place(tag):
        return zm(tag[1]) if tag[0] == 0 else zp(tag[1])

    class ZFirst:
        def __init__(self, own, buf):
            self.own, self.buf = own, buf
            self.left, self.right, self.yl, self.yr, self.yo = {}, {}, {}, {}, {}

        def to_y(self, src, at, tag):
            self.yl[tag] = send(src, self.buf.at[at, y], dev_yr)
            self.yr[tag] = send(src, self.buf.at[at, y], dev_yl)

        def start(self):
            self.left[0] = send(self.own, self.buf.at[z, y], dev_zr)
            self.right[0] = send(self.own, self.buf.at[z, y], dev_zl)
            self.to_y(self.own, z, (0, 0))

        def ring(self, s):
            block = self.buf.at[zm(s), y]
            self.left[s - 1].wait_recv()
            if s < 8:
                self.left[s] = send(block, block, dev_zr)
            if s <= 7:
                block = self.buf.at[zp(s), y]
                self.right[s - 1].wait_recv()
                if s < 7:
                    self.right[s] = send(block, block, dev_zl)
            for tag in tags(s):
                at = place(tag)
                self.to_y(self.buf.at[at, y], at, tag)

        def across(self, s):
            for tag in tags(s):
                at = place(tag)
                rightward = tag[0] == 0 and tag[1] < 8
                self.yl[tag].wait_recv()
                if rightward:
                    self.yo[tag] = send(self.buf.at[at, yl], self.buf.at[at, yl], dev_yr)
                self.yr[tag].wait_recv()
                if not rightward:
                    self.yo[tag] = send(self.buf.at[at, yr], self.buf.at[at, yr], dev_yl)

        def done(self, s):
            for tag in tags(s):
                self.yo[tag].wait_recv()

    class YFirst:
        def __init__(self, own, buf):
            self.own, self.buf = own, buf
            self.left, self.right = {}, {}

        def begin_piece(self, p, col, src):
            self.left[p, 0] = send(src, self.buf.at[z, col], dev_zr)
            self.right[p, 0] = send(src, self.buf.at[z, col], dev_zl)

        def start(self):
            self.from_l = send(self.own, self.buf.at[z, y], dev_yr)
            self.from_r = send(self.own, self.buf.at[z, y], dev_yl)
            self.begin_piece(0, y, self.own)

        def begin(self):
            self.from_l.wait_recv()
            block = self.buf.at[z, yl]
            self.from_o = send(block, block, dev_yr)
            self.begin_piece(1, yl, block)
            self.from_r.wait_recv()
            self.begin_piece(2, yr, self.buf.at[z, yr])

        def begin_last(self):
            self.from_o.wait_recv()
            self.begin_piece(3, yo, self.buf.at[z, yo])

        def ring(self, s):
            for p, col in enumerate((y, yl, yr, yo)):
                self.left[p, s - 1].wait_recv()
                if s < 8:
                    block = self.buf.at[zm(s), col]
                    self.left[p, s] = send(block, block, dev_zr)
                if s <= 7:
                    self.right[p, s - 1].wait_recv()
                    if s < 7:
                        block = self.buf.at[zp(s), col]
                        self.right[p, s] = send(block, block, dev_zl)

    def x_start(src, slot):
        own = slot(x, c)
        return {"l": send(src, own, dev_xr), "r": send(src, own, dev_xl), "p": send(src, own, dev_p)}

    def x_forward(g, slot, halves):
        left, right = slot(xl, c), slot(xr, c)
        g["l"].wait_recv()
        g["a"] = send(halves(left)[0], halves(left)[0], dev_xr)
        g["pl"] = send(left, left, dev_p)
        g["r"].wait_recv()
        g["b"] = send(halves(right)[1], halves(right)[1], dev_xl)
        g["pr"] = send(right, right, dev_p)

    def x_relay(g, slot, halves):
        a, b = halves(slot(xo, c))
        g["a"].wait_recv()
        g["pa"] = send(a, a, dev_p)
        g["b"].wait_recv()
        g["pb"] = send(b, b, dev_p)

    def x_done(g):
        for name in ("p", "pl", "pr", "pa", "pb"):
            g[name].wait_recv()

    def ow_slot(a, b):
        return ow.at[a * NC + b]

    def ow_halves(ref):
        return ref.at[pl.ds(0, 64)], ref.at[pl.ds(64, 64)]

    def att_slot(a, b):
        return att.at[a * NC + b]

    def att_halves(ref):
        return ref.at[pl.ds(0, 192)], ref.at[pl.ds(192, 192)]

    def lane_halves(ref):
        return ref.at[:, pl.ds(0, HALF)], ref.at[:, pl.ds(HALF, HALF)]

    ga = ZFirst(gate_w.at[:, pl.ds(0, MAIN)], wga)
    gb = YFirst(gb_own, wgb)
    dn = ZFirst(dn_own, wd)
    halo = [
        send(key.at[pl.ds(256, 128), lanes], kext.at[pl.ds(0, 128)], dev_after),
        send(value.at[pl.ds(256, 128), lanes], vext.at[pl.ds(0, 128)], dev_after),
        send(dsend.at[0], dext.at[0], dev_after),
        send(key.at[pl.ds(0, 128), lanes], kext.at[pl.ds(512, 128)], dev_before),
        send(value.at[pl.ds(0, 128), lanes], vext.at[pl.ds(512, 128)], dev_before),
        send(dsend.at[1], dext.at[1], dev_before),
    ]
    gb.start()
    ga.start()
    dn.start()
    ow_g = x_start(out_w, ow_slot)
    ow[x * NC + c] = out_w[...]
    gb.begin()

    def attend(block):
        q = query[pl.ds(block * 128, 128), :]
        k = kext[pl.ds(block * 128, 384), :]
        v = vext[pl.ds(block * 128, 384), :]
        scores = lax.dot_general(q, k, (((1,), (1,)), ((), ())), preferred_element_type=F32)
        scores = scores * HD ** (-0.5)
        if block == 0:
            first = jnp.where(sp == 0, -1, dext[0, 0:1])
        else:
            first = docs[block - 1 : block]
        if block == 2:
            last = jnp.where(sp == NZ * NY - 1, -1, dext[1, 0:1])
        else:
            last = docs[block + 1 : block + 2]
        around = jnp.concatenate([first, docs[block : block + 1], last], axis=1)
        mine = jnp.transpose(jnp.broadcast_to(docs[block : block + 1], (128, 128)))[:, 0:1]
        row = lax.broadcasted_iota(jnp.int32, (128, 384), 0)
        col = lax.broadcasted_iota(jnp.int32, (128, 384), 1)
        allowed = (col >= row) & (col <= row + 2 * WIN) & (mine == around)
        masked = jnp.where(allowed, scores, LOW)
        here = sink[0]
        peak = jnp.maximum(jnp.max(masked, axis=1, keepdims=True), here)
        lifted = jnp.where(allowed, jnp.exp(masked - peak), 0.0)
        denom = jnp.sum(lifted, axis=1, keepdims=True) + jnp.exp(here - peak)
        probs = (lifted / denom).astype(BF)
        attended = jnp.dot(probs, v, preferred_element_type=F32).astype(BF)
        att[x * NC + c, pl.ds(block * 128, 128), :] = attended

    def rings(s):
        ga.ring(s)
        dn.ring(s)
        gb.ring(s)

    def across(s):
        ga.across(s)
        dn.across(s)

    attend(1)
    gb.begin_last()
    for copy in halo:
        copy.wait_recv()
    attend(0)
    rings(1)
    attend(2)
    across(0)
    rings(2)
    att_g = x_start(att.at[x * NC + c], att_slot)
    across(1)
    x_forward(ow_g, ow_slot, ow_halves)
    rings(3)
    x_forward(att_g, att_slot, att_halves)
    across(2)
    x_relay(ow_g, ow_slot, ow_halves)
    x_relay(att_g, att_slot, att_halves)
    rings(4)
    across(3)
    x_done(ow_g)
    x_done(att_g)

    def project(n, squares):
        cols = pl.ds(pl.multiple_of(n * 256, 256), 256)
        left = jnp.concatenate([att[h] for h in range(8)], axis=1)
        right = ow[:, :, cols].reshape(1024, 256)
        branch = jnp.dot(left, right, preferred_element_type=F32).astype(BF)
        total = (stream[:, cols].astype(F32) + branch.astype(F32)).astype(BF)
        carried[:, :, cols] = total.reshape(8, OWN, 256)
        wide = total.astype(F32)
        return squares + jnp.sum(wide * wide, axis=1, keepdims=True)

    squares = lax.fori_loop(0, 8, project, jnp.zeros((TOK, 1), F32))
    scale = lax.rsqrt(squares / D + EPS)

    rings(5)

    def normalize(n, carry):
        cols = pl.ds(pl.multiple_of(n * 256, 256), 256)
        wide = carried[:, :, cols].reshape(TOK, 256).astype(F32)
        normed[:, cols] = (wide * scale * gain[:, cols]).astype(BF)
        return carry

    lax.fori_loop(0, 8, normalize, 0)
    across(4)

    def accumulate(za, zb, first):
        left = jnp.concatenate(
            [
                normed[:, pl.ds(pl.multiple_of(za * 128, 128), 128)],
                normed[:, pl.ds(pl.multiple_of(zb * 128, 128), 128)],
            ],
            axis=1,
        )
        for buf, acc, width in ((wga, acc_a, MAIN), (wgb, acc_b, FP)):
            right = jnp.concatenate([buf[za].reshape(128, width), buf[zb].reshape(128, width)], axis=0)
            term = jnp.dot(left, right, preferred_element_type=F32)
            if first:
                acc[...] = term
            else:
                acc[...] += term

    def accumulate_tag(s, first=False):
        accumulate(zm(s), zp(s), first)

    ga.done(1)
    accumulate_tag(1, True)
    rings(6)
    across(5)
    ga.done(2)
    ga.done(3)

    def both(i, carry):
        accumulate_tag(i)
        return carry

    lax.fori_loop(2, 4, both, 0)
    rings(7)
    across(6)
    ga.done(4)
    accumulate_tag(4)
    rings(8)
    across(7)
    ga.done(5)
    accumulate_tag(5)
    ga.done(6)
    accumulate_tag(6)
    across(8)
    ga.done(7)
    accumulate_tag(7)
    ga.done(0)
    ga.done(8)
    accumulate(z, zm(8), False)

    gate, up = acc_a[...], acc_b[:, 0:MAIN]
    hid[:, 0:MAIN] = (gate / (1.0 + jnp.exp(-gate)) * up).astype(BF)
    rest = acc_b[:, MAIN:FP]
    swapped = pltpu.roll(rest, TAIL, 1)
    tail = rest / (1.0 + jnp.exp(-rest)) * swapped
    lane = lax.broadcasted_iota(jnp.int32, (TOK, 2 * TAIL), 1)
    hid[:, MAIN:FP] = jnp.where(lane < TAIL, tail, 0.0).astype(BF)

    own = c * NX + x
    low, high = pl.ds(0, HALF), pl.ds(HALF, HALF)
    chunks = [{} for _ in range(4)]

    def groups(k):
        if k == 3:
            return [zm(7), zp(7), z, zm(8)]
        return [zm(2 * k + 1), zp(2 * k + 1), zm(2 * k + 2), zp(2 * k + 2)]

    def lower(k):
        at = groups(k)
        for i in (0, 2):
            w = jnp.concatenate([wd[at[i]].reshape(128, FP), wd[at[i + 1]].reshape(128, FP)], axis=0)
            term = lax.dot_general(hid[...], w, (((1,), (1,)), ((), ())), preferred_element_type=F32)
            part[k, :, :, :, pl.ds(i * 128, 256)] = term.astype(BF).reshape(NC, NX, OWN, 256)
        chunks[k]["pair"] = send(part.at[k, pc], pair_in.at[k], dev_p)

    def fold(k):
        g = chunks[k]
        g["pair"].wait_recv()
        summed[k] = (part[k, c].astype(F32) + pair_in[k].astype(F32)).astype(BF)
        g["opp_a"] = send(summed.at[k, xo, :, low], opp_in.at[k, 0], dev_xr)
        g["opp_b"] = send(summed.at[k, xo, :, high], opp_in.at[k, 1], dev_xl)
        g["near_b"] = send(summed.at[k, xr, :, high], near_in.at[k, 1], dev_xr)
        g["near_a"] = send(summed.at[k, xl, :, low], near_in.at[k, 0], dev_xl)

    def pass_on(k):
        g = chunks[k]
        g["opp_a"].wait_recv()
        relay[k, 0] = (opp_in[k, 0].astype(F32) + summed[k, xr, :, low].astype(F32)).astype(BF)
        g["far_a"] = send(relay.at[k, 0], far_in.at[k, 0], dev_xr)
        g["opp_b"].wait_recv()
        relay[k, 1] = (opp_in[k, 1].astype(F32) + summed[k, xl, :, high].astype(F32)).astype(BF)
        g["far_b"] = send(relay.at[k, 1], far_in.at[k, 1], dev_xl)

    def slot(k):
        return lambda a, b: shuffled.at[k, b * NX + a]

    def mix(k):
        g = chunks[k]
        base = jnp.concatenate(
            [carried[own, :, pl.ds(pl.multiple_of(at * 128, 128), 128)] for at in groups(k)], axis=1
        ).astype(F32)
        g["near_a"].wait_recv()
        g["near_b"].wait_recv()
        for i, name in ((0, "far_a"), (1, "far_b")):
            g[name].wait_recv()
            cols = pl.ds(i * HALF, HALF)
            feed = summed[k, x, :, cols].astype(F32) + near_in[k, i].astype(F32) + far_in[k, i].astype(F32)
            feed = feed.astype(BF).astype(F32)
            shuffled[k, own, :, cols] = (base[:, i * HALF : (i + 1) * HALF] + 0.5 * feed).astype(BF)
        g["out"] = x_start(shuffled.at[k, own], slot(k))

    def forward(k):
        x_forward(chunks[k]["out"], slot(k), lane_halves)

    def hand_over(k):
        x_relay(chunks[k]["out"], slot(k), lane_halves)

    def write(k):
        x_done(chunks[k]["out"])
        for i, at in enumerate(groups(k)):
            cols = pl.ds(pl.multiple_of(at * 128, 128), 128)
            out[:, :, cols] = shuffled[k, :, :, pl.ds(i * 128, 128)]

    for i in range(1, 7):
        dn.done(i)
    lower(0)
    lower(1)
    fold(0)
    lower(2)
    fold(1)
    dn.done(7)
    dn.done(0)
    dn.done(8)
    lower(3)
    fold(2)
    pass_on(0)
    fold(3)
    pass_on(1)
    mix(0)
    pass_on(2)
    mix(1)
    forward(0)
    pass_on(3)
    mix(2)
    forward(1)
    hand_over(0)
    mix(3)
    forward(2)
    hand_over(1)
    write(0)
    forward(3)
    hand_over(2)
    write(1)
    hand_over(3)
    write(2)
    write(3)
    for copy in started:
        copy.wait_send()


def per_device(
    stream,
    query_rows,
    key_rows,
    value_rows,
    doc_ids,
    sink_logit,
    out_weight,
    norm_gain,
    gate_weight,
    up_weight,
    down_weight,
):
    vmem = pl.BlockSpec(memory_space=pltpu.VMEM)
    smem = pl.BlockSpec(memory_space=pltpu.SMEM)
    result = pl.pallas_call(
        kernel,
        name="layer",
        out_shape=jax.ShapeDtypeStruct((8, OWN, D), BF),
        in_specs=[vmem] * 5 + [smem] + [vmem] * 5,
        out_specs=vmem,
        scratch_shapes=[
            pltpu.VMEM((TOK + 2 * WIN, HD), BF),
            pltpu.VMEM((TOK + 2 * WIN, HD), BF),
            pltpu.VMEM((2, 8, 128), jnp.int32),
            pltpu.VMEM((2, 8, 128), jnp.int32),
            pltpu.VMEM((32, FP), BF),
            pltpu.VMEM((32, FP), BF),
            pltpu.VMEM((NZ, NY, 32, MAIN), BF),
            pltpu.VMEM((NZ, NY, 32, FP), BF),
            pltpu.VMEM((NZ, NY, 32, FP), BF),
            pltpu.VMEM((8, 128, D), BF),
            pltpu.VMEM((8, TOK, HD), BF),
            pltpu.VMEM((8, OWN, D), BF),
            pltpu.VMEM((TOK, D), BF),
            pltpu.VMEM((TOK, MAIN), F32),
            pltpu.VMEM((TOK, FP), F32),
            pltpu.VMEM((TOK, FP), BF),
            pltpu.VMEM((4, NC, NX, OWN, CHUNK), BF),
            pltpu.VMEM((4, NX, OWN, CHUNK), BF),
            pltpu.VMEM((4, NX, OWN, CHUNK), BF),
            pltpu.VMEM((4, 2, OWN, HALF), BF),
            pltpu.VMEM((4, 2, OWN, HALF), BF),
            pltpu.VMEM((4, 2, OWN, HALF), BF),
            pltpu.VMEM((4, 2, OWN, HALF), BF),
            pltpu.VMEM((4, 8, OWN, CHUNK), BF),
            pltpu.SemaphoreType.DMA((COPIES,)),
            pltpu.SemaphoreType.DMA((COPIES,)),
        ],
        compiler_params=pltpu.CompilerParams(
            collective_id=0, has_side_effects=True, vmem_limit_bytes=36 * 1024 * 1024
        ),
    )(
        stream,
        query_rows,
        key_rows,
        value_rows,
        doc_ids.reshape(3, 128),
        sink_logit,
        out_weight,
        norm_gain.reshape(1, D),
        gate_weight,
        up_weight,
        down_weight.T,
    )
    return result.reshape(TOK, D)


def solution(mesh):
    split = Mesh(mesh.devices.reshape(NZ, NY, NX, NC), ("z", "y", "x", "c"))
    placed = (
        P(SP, None),
        P(SP, TP),
        P(SP, None),
        P(SP, None),
        P(SP),
        P(TP),
        P(TP, None),
        P(),
        P(SP, TP),
        P(SP, TP),
        P(TP, SP),
    )
    return jax.shard_map(
        per_device, mesh=split, in_specs=placed, out_specs=P(SP, None), check_vma=False
    )
```

```python
import jax
import jax.numpy as jnp
from jax import lax
from jax.experimental import pallas as pl
from jax.experimental.pallas import tpu as pltpu
from jax.sharding import Mesh
from jax.sharding import PartitionSpec as P

HD = 128
WIN = 128
NZ, NY, NX, NC = 16, 4, 4, 2
TOK = 384
D = 2048
FFL = 704
MAIN = 640
TAIL = 64
FP = 768
OWN = TOK // (NX * NC)
EPS = 1e-06
LOW = -1e30
COPIES = 280
CHUNK = D // 4
HALF = CHUNK // 2
SP = ("z", "y")
TP = ("x", "c")
F32 = jnp.float32
BF = jnp.bfloat16


def kernel(
    far_stream,
    far_query,
    far_key,
    far_value,
    far_docs,
    sink,
    far_out_w,
    far_gain,
    far_gate_w,
    far_up_w,
    far_down_w,
    out,
    stream,
    query,
    key,
    value,
    docs,
    out_w,
    gain,
    gate_w,
    up_w,
    down_w,
    local_sems,
    kext,
    vext,
    dsend,
    dext,
    gb_own,
    dn_own,
    wga,
    wgb,
    wd,
    ow,
    att,
    carried,
    normed,
    acc_a,
    acc_b,
    hid,
    part,
    summed,
    pair_in,
    opp_in,
    relay,
    near_in,
    far_in,
    shuffled,
    send_sems,
    recv_sems,
):
    z, y = lax.axis_index("z"), lax.axis_index("y")
    x, c = lax.axis_index("x"), lax.axis_index("c")
    zr, zl = lax.rem(z + 1, NZ), lax.rem(z + NZ - 1, NZ)
    yr, yl = lax.rem(y + 1, NY), lax.rem(y + NY - 1, NY)
    xr, xl = lax.rem(x + 1, NX), lax.rem(x + NX - 1, NX)
    yo, xo = lax.rem(y + 2, NY), lax.rem(x + 2, NX)
    pc = 1 - c
    sp = z * NY + y
    after, before = lax.rem(sp + 1, NZ * NY), lax.rem(sp + NZ * NY - 1, NZ * NY)
    dev_zr, dev_zl = (zr, y, x, c), (zl, y, x, c)
    dev_yr, dev_yl = (z, yr, x, c), (z, yl, x, c)
    dev_xr, dev_xl = (z, y, xr, c), (z, y, xl, c)
    dev_p = (z, y, x, pc)
    dev_after = (after // NY, lax.rem(after, NY), x, c)
    dev_before = (before // NY, lax.rem(before, NY), x, c)

    barrier = pltpu.get_barrier_semaphore()
    peers = (dev_zr, dev_zl, dev_yr, dev_yl, dev_xr, dev_xl, dev_p, dev_after, dev_before)
    for peer in peers:
        pl.semaphore_signal(barrier, inc=1, device_id=peer, device_id_type=pl.DeviceIdType.MESH)

    local = {}

    def fetch(name, src, dst):
        local[name] = pltpu.make_async_copy(src, dst, local_sems.at[len(local)])
        local[name].start()

    fetch("gate_w", far_gate_w, gate_w)
    fetch("up_w", far_up_w, up_w)
    fetch("down_w", far_down_w, down_w)
    fetch("docs", far_docs, docs)
    fetch("key", far_key, key)
    fetch("value", far_value, value)
    fetch("out_w", far_out_w, out_w)
    fetch("query", far_query, query)
    fetch("gain", far_gain, gain)
    fetch("stream", far_stream, stream)
    local["gate_w"].wait()
    local["up_w"].wait()
    local["down_w"].wait()
    gb_own[:, 0:MAIN] = up_w[:, 0:MAIN]
    gb_own[:, MAIN:FP] = jnp.concatenate([gate_w[:, MAIN:FFL], up_w[:, MAIN:FFL]], axis=1)
    dn_own[:, 0:MAIN] = down_w[:, 0:MAIN]
    dn_own[:, MAIN:FP] = jnp.concatenate([down_w[:, MAIN:FFL], jnp.zeros((32, TAIL), BF)], axis=1)
    local["docs"].wait()
    dsend[0] = jnp.broadcast_to(docs[2:3], (8, 128))
    dsend[1] = jnp.broadcast_to(docs[0:1], (8, 128))
    group = pl.multiple_of((x // 2) * HD, HD)
    lanes = pl.ds(group, HD)
    local["key"].wait()
    local["value"].wait()
    local["out_w"].wait()
    wga[z, y] = gate_w[:, 0:MAIN]

    pl.semaphore_wait(barrier, len(peers))

    started = []

    def send(src, dst, dev):
        at = len(started)
        copy = pltpu.make_async_remote_copy(
            src_ref=src,
            dst_ref=dst,
            send_sem=send_sems.at[at],
            recv_sem=recv_sems.at[at],
            device_id=dev,
            device_id_type=pl.DeviceIdType.MESH,
        )
        copy.start()
        started.append(copy)
        return copy

    def zm(s):
        return lax.rem(z + NZ - s, NZ)

    def zp(s):
        return lax.rem(z + s, NZ)

    def tags(s):
        if s == 0:
            return [(0, 0)]
        if s == 8:
            return [(0, 8)]
        return [(0, s), (1, s)]

    def place(tag):
        return zm(tag[1]) if tag[0] == 0 else zp(tag[1])

    class ZFirst:
        def __init__(self, own, buf):
            self.own, self.buf = own, buf
            self.left, self.right, self.yl, self.yr, self.yo = {}, {}, {}, {}, {}

        def to_y(self, src, at, tag):
            self.yl[tag] = send(src, self.buf.at[at, y], dev_yr)
            self.yr[tag] = send(src, self.buf.at[at, y], dev_yl)

        def start(self):
            self.left[0] = send(self.own, self.buf.at[z, y], dev_zr)
            self.right[0] = send(self.own, self.buf.at[z, y], dev_zl)
            self.to_y(self.own, z, (0, 0))

        def ring(self, s):
            block = self.buf.at[zm(s), y]
            self.left[s - 1].wait_recv()
            if s < 8:
                self.left[s] = send(block, block, dev_zr)
            if s <= 7:
                block = self.buf.at[zp(s), y]
                self.right[s - 1].wait_recv()
                if s < 7:
                    self.right[s] = send(block, block, dev_zl)
            for tag in tags(s):
                at = place(tag)
                self.to_y(self.buf.at[at, y], at, tag)

        def across(self, s):
            for tag in tags(s):
                at = place(tag)
                rightward = tag[0] == 0 and tag[1] < 8
                self.yl[tag].wait_recv()
                if rightward:
                    self.yo[tag] = send(self.buf.at[at, yl], self.buf.at[at, yl], dev_yr)
                self.yr[tag].wait_recv()
                if not rightward:
                    self.yo[tag] = send(self.buf.at[at, yr], self.buf.at[at, yr], dev_yl)

        def done(self, s):
            for tag in tags(s):
                self.yo[tag].wait_recv()

    class YFirst:
        def __init__(self, own, buf):
            self.own, self.buf = own, buf
            self.left, self.right = {}, {}

        def begin_piece(self, p, col, src):
            self.left[p, 0] = send(src, self.buf.at[z, col], dev_zr)
            self.right[p, 0] = send(src, self.buf.at[z, col], dev_zl)

        def start(self):
            self.from_l = send(self.own, self.buf.at[z, y], dev_yr)
            self.from_r = send(self.own, self.buf.at[z, y], dev_yl)
            self.begin_piece(0, y, self.own)

        def begin(self):
            self.from_l.wait_recv()
            block = self.buf.at[z, yl]
            self.from_o = send(block, block, dev_yr)
            self.begin_piece(1, yl, block)
            self.from_r.wait_recv()
            self.begin_piece(2, yr, self.buf.at[z, yr])

        def begin_last(self):
            self.from_o.wait_recv()
            self.begin_piece(3, yo, self.buf.at[z, yo])

        def ring(self, s):
            for p, col in enumerate((y, yl, yr, yo)):
                self.left[p, s - 1].wait_recv()
                if s < 8:
                    block = self.buf.at[zm(s), col]
                    self.left[p, s] = send(block, block, dev_zr)
                if s <= 7:
                    self.right[p, s - 1].wait_recv()
                    if s < 7:
                        block = self.buf.at[zp(s), col]
                        self.right[p, s] = send(block, block, dev_zl)

    def x_start(src, slot):
        own = slot(x, c)
        return {"l": send(src, own, dev_xr), "r": send(src, own, dev_xl), "p": send(src, own, dev_p)}

    def x_forward(g, slot, halves):
        left, right = slot(xl, c), slot(xr, c)
        g["l"].wait_recv()
        g["a"] = send(halves(left)[0], halves(left)[0], dev_xr)
        g["pl"] = send(left, left, dev_p)
        g["r"].wait_recv()
        g["b"] = send(halves(right)[1], halves(right)[1], dev_xl)
        g["pr"] = send(right, right, dev_p)

    def x_relay(g, slot, halves):
        a, b = halves(slot(xo, c))
        g["a"].wait_recv()
        g["pa"] = send(a, a, dev_p)
        g["b"].wait_recv()
        g["pb"] = send(b, b, dev_p)

    def x_done(g):
        for name in ("p", "pl", "pr", "pa", "pb"):
            g[name].wait_recv()

    def ow_slot(a, b):
        return ow.at[a * NC + b]

    def ow_halves(ref):
        return ref.at[pl.ds(0, 64)], ref.at[pl.ds(64, 64)]

    def att_slot(a, b):
        return att.at[a * NC + b]

    def att_halves(ref):
        return ref.at[pl.ds(0, 192)], ref.at[pl.ds(192, 192)]

    def lane_halves(ref):
        return ref.at[:, pl.ds(0, HALF)], ref.at[:, pl.ds(HALF, HALF)]

    ga = ZFirst(gate_w.at[:, pl.ds(0, MAIN)], wga)
    gb = YFirst(gb_own, wgb)
    dn = ZFirst(dn_own, wd)
    halo = [
        send(key.at[pl.ds(256, 128), lanes], kext.at[pl.ds(0, 128)], dev_after),
        send(value.at[pl.ds(256, 128), lanes], vext.at[pl.ds(0, 128)], dev_after),
        send(dsend.at[0], dext.at[0], dev_after),
        send(key.at[pl.ds(0, 128), lanes], kext.at[pl.ds(512, 128)], dev_before),
        send(value.at[pl.ds(0, 128), lanes], vext.at[pl.ds(512, 128)], dev_before),
        send(dsend.at[1], dext.at[1], dev_before),
    ]
    gb.start()
    ga.start()
    dn.start()
    ow_g = x_start(out_w, ow_slot)
    ow[x * NC + c] = out_w[...]
    wgb[z, y] = gb_own[...]
    wd[z, y] = dn_own[...]
    kext[pl.ds(128, 384), :] = key[:, lanes]
    vext[pl.ds(128, 384), :] = value[:, lanes]
    local["query"].wait()
    gb.begin()

    def attend(block):
        q = query[pl.ds(block * 128, 128), :]
        k = kext[pl.ds(block * 128, 384), :]
        v = vext[pl.ds(block * 128, 384), :]
        scores = lax.dot_general(q, k, (((1,), (1,)), ((), ())), preferred_element_type=F32)
        scores = scores * HD ** (-0.5)
        if block == 0:
            first = jnp.where(sp == 0, -1, dext[0, 0:1])
        else:
            first = docs[block - 1 : block]
        if block == 2:
            last = jnp.where(sp == NZ * NY - 1, -1, dext[1, 0:1])
        else:
            last = docs[block + 1 : block + 2]
        around = jnp.concatenate([first, docs[block : block + 1], last], axis=1)
        mine = jnp.transpose(jnp.broadcast_to(docs[block : block + 1], (128, 128)))[:, 0:1]
        row = lax.broadcasted_iota(jnp.int32, (128, 384), 0)
        col = lax.broadcasted_iota(jnp.int32, (128, 384), 1)
        allowed = (col >= row) & (col <= row + 2 * WIN) & (mine == around)
        masked = jnp.where(allowed, scores, LOW)
        here = sink[0]
        peak = jnp.maximum(jnp.max(masked, axis=1, keepdims=True), here)
        lifted = jnp.where(allowed, jnp.exp(masked - peak), 0.0)
        denom = jnp.sum(lifted, axis=1, keepdims=True) + jnp.exp(here - peak)
        probs = (lifted / denom).astype(BF)
        attended = jnp.dot(probs, v, preferred_element_type=F32).astype(BF)
        att[x * NC + c, pl.ds(block * 128, 128), :] = attended

    def rings(s):
        ga.ring(s)
        dn.ring(s)
        gb.ring(s)

    def across(s):
        ga.across(s)
        dn.across(s)

    attend(1)
    gb.begin_last()
    for copy in halo:
        copy.wait_recv()
    attend(0)
    rings(1)
    attend(2)
    across(0)
    rings(2)
    att_g = x_start(att.at[x * NC + c], att_slot)
    across(1)
    x_forward(ow_g, ow_slot, ow_halves)
    rings(3)
    x_forward(att_g, att_slot, att_halves)
    across(2)
    x_relay(ow_g, ow_slot, ow_halves)
    x_relay(att_g, att_slot, att_halves)
    rings(4)
    across(3)
    x_done(ow_g)
    x_done(att_g)

    local["gain"].wait()
    local["stream"].wait()

    def project(n, squares):
        cols = pl.ds(pl.multiple_of(n * 256, 256), 256)
        left = jnp.concatenate([att[h] for h in range(8)], axis=1)
        right = ow[:, :, cols].reshape(1024, 256)
        branch = jnp.dot(left, right, preferred_element_type=F32).astype(BF)
        total = (stream[:, cols].astype(F32) + branch.astype(F32)).astype(BF)
        carried[:, :, cols] = total.reshape(8, OWN, 256)
        wide = total.astype(F32)
        return squares + jnp.sum(wide * wide, axis=1, keepdims=True)

    squares = lax.fori_loop(0, 8, project, jnp.zeros((TOK, 1), F32))
    scale = lax.rsqrt(squares / D + EPS)

    rings(5)

    def normalize(n, carry):
        cols = pl.ds(pl.multiple_of(n * 256, 256), 256)
        wide = carried[:, :, cols].reshape(TOK, 256).astype(F32)
        normed[:, cols] = (wide * scale * gain[:, cols]).astype(BF)
        return carry

    lax.fori_loop(0, 8, normalize, 0)
    across(4)

    def accumulate(za, zb, first):
        left = jnp.concatenate(
            [
                normed[:, pl.ds(pl.multiple_of(za * 128, 128), 128)],
                normed[:, pl.ds(pl.multiple_of(zb * 128, 128), 128)],
            ],
            axis=1,
        )
        for buf, acc, width in ((wga, acc_a, MAIN), (wgb, acc_b, FP)):
            right = jnp.concatenate([buf[za].reshape(128, width), buf[zb].reshape(128, width)], axis=0)
            term = jnp.dot(left, right, preferred_element_type=F32)
            if first:
                acc[...] = term
            else:
                acc[...] += term

    def accumulate_tag(s, first=False):
        accumulate(zm(s), zp(s), first)

    ga.done(1)
    accumulate_tag(1, True)
    rings(6)
    across(5)
    ga.done(2)
    ga.done(3)

    def both(i, carry):
        accumulate_tag(i)
        return carry

    lax.fori_loop(2, 4, both, 0)
    rings(7)
    across(6)
    ga.done(4)
    accumulate_tag(4)
    rings(8)
    across(7)
    ga.done(5)
    accumulate_tag(5)
    ga.done(6)
    accumulate_tag(6)
    across(8)
    ga.done(7)
    accumulate_tag(7)
    ga.done(0)
    ga.done(8)
    accumulate(z, zm(8), False)

    gate, up = acc_a[...], acc_b[:, 0:MAIN]
    hid[:, 0:MAIN] = (gate / (1.0 + jnp.exp(-gate)) * up).astype(BF)
    rest = acc_b[:, MAIN:FP]
    swapped = pltpu.roll(rest, TAIL, 1)
    tail = rest / (1.0 + jnp.exp(-rest)) * swapped
    lane = lax.broadcasted_iota(jnp.int32, (TOK, 2 * TAIL), 1)
    hid[:, MAIN:FP] = jnp.where(lane < TAIL, tail, 0.0).astype(BF)

    own = c * NX + x
    low, high = pl.ds(0, HALF), pl.ds(HALF, HALF)
    chunks = [{} for _ in range(4)]

    def groups(k):
        if k == 3:
            return [zm(7), zp(7), z, zm(8)]
        return [zm(2 * k + 1), zp(2 * k + 1), zm(2 * k + 2), zp(2 * k + 2)]

    def lower(k):
        at = groups(k)
        for i in (0, 2):
            w = jnp.concatenate([wd[at[i]].reshape(128, FP), wd[at[i + 1]].reshape(128, FP)], axis=0)
            term = lax.dot_general(hid[...], w, (((1,), (1,)), ((), ())), preferred_element_type=F32)
            part[k, :, :, :, pl.ds(i * 128, 256)] = term.astype(BF).reshape(NC, NX, OWN, 256)
        chunks[k]["pair"] = send(part.at[k, pc], pair_in.at[k], dev_p)

    def fold(k):
        g = chunks[k]
        g["pair"].wait_recv()
        summed[k] = (part[k, c].astype(F32) + pair_in[k].astype(F32)).astype(BF)
        g["opp_a"] = send(summed.at[k, xo, :, low], opp_in.at[k, 0], dev_xr)
        g["opp_b"] = send(summed.at[k, xo, :, high], opp_in.at[k, 1], dev_xl)
        g["near_b"] = send(summed.at[k, xr, :, high], near_in.at[k, 1], dev_xr)
        g["near_a"] = send(summed.at[k, xl, :, low], near_in.at[k, 0], dev_xl)

    def pass_on(k):
        g = chunks[k]
        g["opp_a"].wait_recv()
        relay[k, 0] = (opp_in[k, 0].astype(F32) + summed[k, xr, :, low].astype(F32)).astype(BF)
        g["far_a"] = send(relay.at[k, 0], far_in.at[k, 0], dev_xr)
        g["opp_b"].wait_recv()
        relay[k, 1] = (opp_in[k, 1].astype(F32) + summed[k, xl, :, high].astype(F32)).astype(BF)
        g["far_b"] = send(relay.at[k, 1], far_in.at[k, 1], dev_xl)

    def slot(k):
        return lambda a, b: shuffled.at[k, b * NX + a]

    def mix(k):
        g = chunks[k]
        base = jnp.concatenate(
            [carried[own, :, pl.ds(pl.multiple_of(at * 128, 128), 128)] for at in groups(k)], axis=1
        ).astype(F32)
        g["near_a"].wait_recv()
        g["near_b"].wait_recv()
        for i, name in ((0, "far_a"), (1, "far_b")):
            g[name].wait_recv()
            cols = pl.ds(i * HALF, HALF)
            feed = summed[k, x, :, cols].astype(F32) + near_in[k, i].astype(F32) + far_in[k, i].astype(F32)
            feed = feed.astype(BF).astype(F32)
            shuffled[k, own, :, cols] = (base[:, i * HALF : (i + 1) * HALF] + 0.5 * feed).astype(BF)
        g["out"] = x_start(shuffled.at[k, own], slot(k))

    def forward(k):
        x_forward(chunks[k]["out"], slot(k), lane_halves)

    def hand_over(k):
        x_relay(chunks[k]["out"], slot(k), lane_halves)

    def write(k):
        x_done(chunks[k]["out"])
        for i, at in enumerate(groups(k)):
            cols = pl.ds(pl.multiple_of(at * 128, 128), 128)
            out[:, :, cols] = shuffled[k, :, :, pl.ds(i * 128, 128)]

    for i in range(1, 7):
        dn.done(i)
    lower(0)
    lower(1)
    fold(0)
    lower(2)
    fold(1)
    dn.done(7)
    dn.done(0)
    dn.done(8)
    lower(3)
    fold(2)
    pass_on(0)
    fold(3)
    pass_on(1)
    mix(0)
    pass_on(2)
    mix(1)
    forward(0)
    pass_on(3)
    mix(2)
    forward(1)
    hand_over(0)
    mix(3)
    forward(2)
    hand_over(1)
    write(0)
    forward(3)
    hand_over(2)
    write(1)
    hand_over(3)
    write(2)
    write(3)
    for copy in started:
        copy.wait_send()


def per_device(
    stream,
    query_rows,
    key_rows,
    value_rows,
    doc_ids,
    sink_logit,
    out_weight,
    norm_gain,
    gate_weight,
    up_weight,
    down_weight,
):
    vmem = pl.BlockSpec(memory_space=pltpu.VMEM)
    smem = pl.BlockSpec(memory_space=pltpu.SMEM)
    far = pl.BlockSpec(memory_space=pltpu.HBM)
    result = pl.pallas_call(
        kernel,
        name="layer",
        out_shape=pltpu.VMEM((8, OWN, D), BF),
        in_specs=[far] * 5 + [smem] + [far] * 5,
        out_specs=vmem,
        scratch_shapes=[
            pltpu.VMEM((TOK, D), BF),
            pltpu.VMEM((TOK, HD), BF),
            pltpu.VMEM((TOK, 2 * HD), BF),
            pltpu.VMEM((TOK, 2 * HD), BF),
            pltpu.VMEM((3, 128), jnp.int32),
            pltpu.VMEM((128, D), BF),
            pltpu.VMEM((1, D), F32),
            pltpu.VMEM((32, FFL), BF),
            pltpu.VMEM((32, FFL), BF),
            pltpu.VMEM((32, FFL), BF),
            pltpu.SemaphoreType.DMA((10,)),
            pltpu.VMEM((TOK + 2 * WIN, HD), BF),
            pltpu.VMEM((TOK + 2 * WIN, HD), BF),
            pltpu.VMEM((2, 8, 128), jnp.int32),
            pltpu.VMEM((2, 8, 128), jnp.int32),
            pltpu.VMEM((32, FP), BF),
            pltpu.VMEM((32, FP), BF),
            pltpu.VMEM((NZ, NY, 32, MAIN), BF),
            pltpu.VMEM((NZ, NY, 32, FP), BF),
            pltpu.VMEM((NZ, NY, 32, FP), BF),
            pltpu.VMEM((8, 128, D), BF),
            pltpu.VMEM((8, TOK, HD), BF),
            pltpu.VMEM((8, OWN, D), BF),
            pltpu.VMEM((TOK, D), BF),
            pltpu.VMEM((TOK, MAIN), F32),
            pltpu.VMEM((TOK, FP), F32),
            pltpu.VMEM((TOK, FP), BF),
            pltpu.VMEM((4, NC, NX, OWN, CHUNK), BF),
            pltpu.VMEM((4, NX, OWN, CHUNK), BF),
            pltpu.VMEM((4, NX, OWN, CHUNK), BF),
            pltpu.VMEM((4, 2, OWN, HALF), BF),
            pltpu.VMEM((4, 2, OWN, HALF), BF),
            pltpu.VMEM((4, 2, OWN, HALF), BF),
            pltpu.VMEM((4, 2, OWN, HALF), BF),
            pltpu.VMEM((4, 8, OWN, CHUNK), BF),
            pltpu.SemaphoreType.DMA((COPIES,)),
            pltpu.SemaphoreType.DMA((COPIES,)),
        ],
        compiler_params=pltpu.CompilerParams(
            collective_id=0, has_side_effects=True, vmem_limit_bytes=60 * 1024 * 1024
        ),
    )(
        stream,
        query_rows,
        key_rows,
        value_rows,
        doc_ids.reshape(3, 128),
        sink_logit,
        out_weight,
        norm_gain.reshape(1, D),
        gate_weight,
        up_weight,
        down_weight.T,
    )
    return result.reshape(TOK, D)


def solution(mesh):
    split = Mesh(mesh.devices.reshape(NZ, NY, NX, NC), ("z", "y", "x", "c"))
    placed = (
        P(SP, None),
        P(SP, TP),
        P(SP, None),
        P(SP, None),
        P(SP),
        P(TP),
        P(TP, None),
        P(),
        P(SP, TP),
        P(SP, TP),
        P(TP, SP),
    )
    return jax.shard_map(
        per_device, mesh=split, in_specs=placed, out_specs=P(SP, None), check_vma=False
    )
```

```python
import jax
import jax.numpy as jnp
from jax import lax
from jax.experimental import pallas as pl
from jax.experimental.pallas import tpu as pltpu
from jax.sharding import Mesh
from jax.sharding import PartitionSpec as P

HD = 128
WIN = 128
NZ, NY, NX, NC = 16, 4, 4, 2
TOK = 384
D = 2048
FFL = 704
MAIN = 640
TAIL = 64
FP = 768
OWN = TOK // (NX * NC)
EPS = 1e-06
LOW = -1e30
COPIES = 280
CHUNK = D // 4
HALF = CHUNK // 2
SP = ("z", "y")
TP = ("x", "c")
F32 = jnp.float32
BF = jnp.bfloat16


def kernel(
    far_stream,
    far_query,
    far_key,
    far_value,
    far_docs,
    sink,
    far_out_w,
    far_gain,
    far_gate_w,
    far_up_w,
    far_down_w,
    out,
    stream,
    query,
    key,
    value,
    docs,
    out_w,
    gain,
    gate_w,
    up_w,
    down_w,
    local_sems,
    kext,
    vext,
    dsend,
    dext,
    gb_own,
    dn_own,
    wga,
    wgb,
    wd,
    ow,
    att,
    carried,
    normed,
    acc_a,
    acc_b,
    hid,
    part,
    summed,
    pair_in,
    opp_in,
    relay,
    near_in,
    far_in,
    shuffled,
    send_sems,
    recv_sems,
):
    z, y = lax.axis_index("z"), lax.axis_index("y")
    x, c = lax.axis_index("x"), lax.axis_index("c")
    zr, zl = lax.rem(z + 1, NZ), lax.rem(z + NZ - 1, NZ)
    yr, yl = lax.rem(y + 1, NY), lax.rem(y + NY - 1, NY)
    xr, xl = lax.rem(x + 1, NX), lax.rem(x + NX - 1, NX)
    yo, xo = lax.rem(y + 2, NY), lax.rem(x + 2, NX)
    pc = 1 - c
    sp = z * NY + y
    after, before = lax.rem(sp + 1, NZ * NY), lax.rem(sp + NZ * NY - 1, NZ * NY)
    dev_zr, dev_zl = (zr, y, x, c), (zl, y, x, c)
    dev_yr, dev_yl = (z, yr, x, c), (z, yl, x, c)
    dev_xr, dev_xl = (z, y, xr, c), (z, y, xl, c)
    dev_p = (z, y, x, pc)
    dev_after = (after // NY, lax.rem(after, NY), x, c)
    dev_before = (before // NY, lax.rem(before, NY), x, c)

    barrier = pltpu.get_barrier_semaphore()
    peers = (dev_zr, dev_zl, dev_yr, dev_yl, dev_xr, dev_xl, dev_p, dev_after, dev_before)
    for peer in peers:
        pl.semaphore_signal(barrier, inc=1, device_id=peer, device_id_type=pl.DeviceIdType.MESH)

    local = {}

    def fetch(name, src, dst):
        local[name] = pltpu.make_async_copy(src, dst, local_sems.at[len(local)])
        local[name].start()

    fetch("gate_w", far_gate_w, gate_w)
    fetch("up_w", far_up_w, up_w)
    fetch("down_w", far_down_w, down_w)
    fetch("docs", far_docs, docs)
    fetch("key", far_key, key)
    fetch("value", far_value, value)
    fetch("out_w", far_out_w, out_w)
    fetch("query", far_query, query)
    fetch("gain", far_gain, gain)
    fetch("stream", far_stream, stream)
    local["gate_w"].wait()
    local["up_w"].wait()
    local["down_w"].wait()
    gb_own[:, 0:MAIN] = up_w[:, 0:MAIN]
    gb_own[:, MAIN:FP] = jnp.concatenate([gate_w[:, MAIN:FFL], up_w[:, MAIN:FFL]], axis=1)
    dn_own[:, 0:MAIN] = down_w[:, 0:MAIN]
    dn_own[:, MAIN:FP] = jnp.concatenate([down_w[:, MAIN:FFL], jnp.zeros((32, TAIL), BF)], axis=1)
    local["docs"].wait()
    dsend[0] = jnp.broadcast_to(docs[2:3], (8, 128))
    dsend[1] = jnp.broadcast_to(docs[0:1], (8, 128))
    group = pl.multiple_of((x // 2) * HD, HD)
    lanes = pl.ds(group, HD)
    local["key"].wait()
    local["value"].wait()
    local["out_w"].wait()
    wga[z, y] = gate_w[:, 0:MAIN]

    pl.semaphore_wait(barrier, len(peers))

    started = []

    def send(src, dst, dev):
        at = len(started)
        copy = pltpu.make_async_remote_copy(
            src_ref=src,
            dst_ref=dst,
            send_sem=send_sems.at[at],
            recv_sem=recv_sems.at[at],
            device_id=dev,
            device_id_type=pl.DeviceIdType.MESH,
        )
        copy.start()
        started.append(copy)
        return copy

    def zm(s):
        return lax.rem(z + NZ - s, NZ)

    def zp(s):
        return lax.rem(z + s, NZ)

    def tags(s):
        if s == 0:
            return [(0, 0)]
        if s == 8:
            return [(0, 8)]
        return [(0, s), (1, s)]

    def place(tag):
        return zm(tag[1]) if tag[0] == 0 else zp(tag[1])

    class ZFirst:
        def __init__(self, own, buf):
            self.own, self.buf = own, buf
            self.left, self.right, self.yl, self.yr, self.yo = {}, {}, {}, {}, {}

        def to_y(self, src, at, tag):
            self.yl[tag] = send(src, self.buf.at[at, y], dev_yr)
            self.yr[tag] = send(src, self.buf.at[at, y], dev_yl)

        def start(self):
            self.left[0] = send(self.own, self.buf.at[z, y], dev_zr)
            self.right[0] = send(self.own, self.buf.at[z, y], dev_zl)
            self.to_y(self.own, z, (0, 0))

        def ring(self, s):
            block = self.buf.at[zm(s), y]
            self.left[s - 1].wait_recv()
            if s < 8:
                self.left[s] = send(block, block, dev_zr)
            if s <= 7:
                block = self.buf.at[zp(s), y]
                self.right[s - 1].wait_recv()
                if s < 7:
                    self.right[s] = send(block, block, dev_zl)
            for tag in tags(s):
                at = place(tag)
                self.to_y(self.buf.at[at, y], at, tag)

        def across(self, s):
            for tag in tags(s):
                at = place(tag)
                rightward = tag[0] == 0 and tag[1] < 8
                self.yl[tag].wait_recv()
                if rightward:
                    self.yo[tag] = send(self.buf.at[at, yl], self.buf.at[at, yl], dev_yr)
                self.yr[tag].wait_recv()
                if not rightward:
                    self.yo[tag] = send(self.buf.at[at, yr], self.buf.at[at, yr], dev_yl)

        def done(self, s):
            for tag in tags(s):
                self.yo[tag].wait_recv()

    class YFirst:
        def __init__(self, own, buf):
            self.own, self.buf = own, buf
            self.left, self.right = {}, {}

        def begin_piece(self, p, col, src):
            self.left[p, 0] = send(src, self.buf.at[z, col], dev_zr)
            self.right[p, 0] = send(src, self.buf.at[z, col], dev_zl)

        def start(self):
            self.from_l = send(self.own, self.buf.at[z, y], dev_yr)
            self.from_r = send(self.own, self.buf.at[z, y], dev_yl)
            self.begin_piece(0, y, self.own)

        def begin(self):
            self.from_l.wait_recv()
            block = self.buf.at[z, yl]
            self.from_o = send(block, block, dev_yr)
            self.begin_piece(1, yl, block)
            self.from_r.wait_recv()
            self.begin_piece(2, yr, self.buf.at[z, yr])

        def begin_last(self):
            self.from_o.wait_recv()
            self.begin_piece(3, yo, self.buf.at[z, yo])

        def ring(self, s):
            for p, col in enumerate((y, yl, yr, yo)):
                self.left[p, s - 1].wait_recv()
                if s < 8:
                    block = self.buf.at[zm(s), col]
                    self.left[p, s] = send(block, block, dev_zr)
                if s <= 7:
                    self.right[p, s - 1].wait_recv()
                    if s < 7:
                        block = self.buf.at[zp(s), col]
                        self.right[p, s] = send(block, block, dev_zl)

    def x_start(src, slot):
        own = slot(x, c)
        return {"l": send(src, own, dev_xr), "r": send(src, own, dev_xl), "p": send(src, own, dev_p)}

    def x_forward(g, slot, halves):
        left, right = slot(xl, c), slot(xr, c)
        g["l"].wait_recv()
        g["a"] = send(halves(left)[0], halves(left)[0], dev_xr)
        g["pl"] = send(left, left, dev_p)
        g["r"].wait_recv()
        g["b"] = send(halves(right)[1], halves(right)[1], dev_xl)
        g["pr"] = send(right, right, dev_p)

    def x_relay(g, slot, halves):
        a, b = halves(slot(xo, c))
        g["a"].wait_recv()
        g["pa"] = send(a, a, dev_p)
        g["b"].wait_recv()
        g["pb"] = send(b, b, dev_p)

    def x_done(g):
        for name in ("p", "pl", "pr", "pa", "pb"):
            g[name].wait_recv()

    def ow_slot(a, b):
        return ow.at[a * NC + b]

    def ow_halves(ref):
        return ref.at[pl.ds(0, 64)], ref.at[pl.ds(64, 64)]

    def att_slot(a, b):
        return att.at[a * NC + b]

    def att_halves(ref):
        return ref.at[pl.ds(0, 192)], ref.at[pl.ds(192, 192)]

    def lane_halves(ref):
        return ref.at[:, pl.ds(0, HALF)], ref.at[:, pl.ds(HALF, HALF)]

    ga = ZFirst(gate_w.at[:, pl.ds(0, MAIN)], wga)
    gb = YFirst(gb_own, wgb)
    dn = ZFirst(dn_own, wd)
    gb.start()
    ga.start()
    dn.start()
    halo = [
        send(key.at[pl.ds(256, 128), lanes], kext.at[pl.ds(0, 128)], dev_after),
        send(value.at[pl.ds(256, 128), lanes], vext.at[pl.ds(0, 128)], dev_after),
        send(dsend.at[0], dext.at[0], dev_after),
        send(key.at[pl.ds(0, 128), lanes], kext.at[pl.ds(512, 128)], dev_before),
        send(value.at[pl.ds(0, 128), lanes], vext.at[pl.ds(512, 128)], dev_before),
        send(dsend.at[1], dext.at[1], dev_before),
    ]
    ow_g = x_start(out_w, ow_slot)
    ow[x * NC + c] = out_w[...]
    wgb[z, y] = gb_own[...]
    wd[z, y] = dn_own[...]
    kext[pl.ds(128, 384), :] = key[:, lanes]
    vext[pl.ds(128, 384), :] = value[:, lanes]
    local["query"].wait()
    gb.begin()

    def attend(block):
        q = query[pl.ds(block * 128, 128), :]
        k = kext[pl.ds(block * 128, 384), :]
        v = vext[pl.ds(block * 128, 384), :]
        scores = lax.dot_general(q, k, (((1,), (1,)), ((), ())), preferred_element_type=F32)
        scores = scores * HD ** (-0.5)
        if block == 0:
            first = jnp.where(sp == 0, -1, dext[0, 0:1])
        else:
            first = docs[block - 1 : block]
        if block == 2:
            last = jnp.where(sp == NZ * NY - 1, -1, dext[1, 0:1])
        else:
            last = docs[block + 1 : block + 2]
        around = jnp.concatenate([first, docs[block : block + 1], last], axis=1)
        mine = jnp.transpose(jnp.broadcast_to(docs[block : block + 1], (128, 128)))[:, 0:1]
        row = lax.broadcasted_iota(jnp.int32, (128, 384), 0)
        col = lax.broadcasted_iota(jnp.int32, (128, 384), 1)
        allowed = (col >= row) & (col <= row + 2 * WIN) & (mine == around)
        masked = jnp.where(allowed, scores, LOW)
        here = sink[0]
        peak = jnp.maximum(jnp.max(masked, axis=1, keepdims=True), here)
        lifted = jnp.where(allowed, jnp.exp(masked - peak), 0.0)
        denom = jnp.sum(lifted, axis=1, keepdims=True) + jnp.exp(here - peak)
        probs = (lifted / denom).astype(BF)
        attended = jnp.dot(probs, v, preferred_element_type=F32).astype(BF)
        att[x * NC + c, pl.ds(block * 128, 128), :] = attended

    def rings(s):
        ga.ring(s)
        ga.across(s - 1)
        dn.ring(s)
        dn.across(s - 1)
        gb.ring(s)

    attend(1)
    gb.begin_last()
    for copy in halo:
        copy.wait_recv()
    attend(0)
    rings(1)
    attend(2)
    rings(2)
    att_g = x_start(att.at[x * NC + c], att_slot)
    x_forward(ow_g, ow_slot, ow_halves)
    rings(3)
    x_forward(att_g, att_slot, att_halves)
    x_relay(ow_g, ow_slot, ow_halves)
    x_relay(att_g, att_slot, att_halves)
    rings(4)
    x_done(ow_g)
    x_done(att_g)

    local["gain"].wait()
    local["stream"].wait()

    def project(n, squares):
        cols = pl.ds(pl.multiple_of(n * 256, 256), 256)
        left = jnp.concatenate([att[h] for h in range(8)], axis=1)
        right = ow[:, :, cols].reshape(1024, 256)
        branch = jnp.dot(left, right, preferred_element_type=F32).astype(BF)
        total = (stream[:, cols].astype(F32) + branch.astype(F32)).astype(BF)
        carried[:, :, cols] = total.reshape(8, OWN, 256)
        wide = total.astype(F32)
        return squares + jnp.sum(wide * wide, axis=1, keepdims=True)

    squares = lax.fori_loop(0, 8, project, jnp.zeros((TOK, 1), F32))
    scale = lax.rsqrt(squares / D + EPS)

    rings(5)

    def normalize(n, carry):
        cols = pl.ds(pl.multiple_of(n * 256, 256), 256)
        wide = carried[:, :, cols].reshape(TOK, 256).astype(F32)
        normed[:, cols] = (wide * scale * gain[:, cols]).astype(BF)
        return carry

    lax.fori_loop(0, 8, normalize, 0)

    def accumulate(za, zb, first):
        left = jnp.concatenate(
            [
                normed[:, pl.ds(pl.multiple_of(za * 128, 128), 128)],
                normed[:, pl.ds(pl.multiple_of(zb * 128, 128), 128)],
            ],
            axis=1,
        )
        for buf, acc, width in ((wga, acc_a, MAIN), (wgb, acc_b, FP)):
            right = jnp.concatenate([buf[za].reshape(128, width), buf[zb].reshape(128, width)], axis=0)
            term = jnp.dot(left, right, preferred_element_type=F32)
            if first:
                acc[...] = term
            else:
                acc[...] += term

    def accumulate_tag(s, first=False):
        accumulate(zm(s), zp(s), first)

    ga.done(1)
    accumulate_tag(1, True)
    rings(6)
    ga.done(2)
    ga.done(3)

    def both(i, carry):
        accumulate_tag(i)
        return carry

    lax.fori_loop(2, 4, both, 0)
    rings(7)
    ga.done(4)
    accumulate_tag(4)
    rings(8)
    ga.done(5)
    accumulate_tag(5)
    ga.done(6)
    accumulate_tag(6)
    ga.across(8)
    dn.across(8)
    ga.done(7)
    accumulate_tag(7)
    ga.done(0)
    ga.done(8)
    accumulate(z, zm(8), False)

    gate, up = acc_a[...], acc_b[:, 0:MAIN]
    hid[:, 0:MAIN] = (gate / (1.0 + jnp.exp(-gate)) * up).astype(BF)
    rest = acc_b[:, MAIN:FP]
    swapped = pltpu.roll(rest, TAIL, 1)
    tail = rest / (1.0 + jnp.exp(-rest)) * swapped
    lane = lax.broadcasted_iota(jnp.int32, (TOK, 2 * TAIL), 1)
    hid[:, MAIN:FP] = jnp.where(lane < TAIL, tail, 0.0).astype(BF)

    own = c * NX + x
    low, high = pl.ds(0, HALF), pl.ds(HALF, HALF)
    chunks = [{} for _ in range(4)]

    def groups(k):
        if k == 3:
            return [zm(7), zp(7), z, zm(8)]
        return [zm(2 * k + 1), zp(2 * k + 1), zm(2 * k + 2), zp(2 * k + 2)]

    def lower(k):
        at = groups(k)
        for i in (0, 2):
            w = jnp.concatenate([wd[at[i]].reshape(128, FP), wd[at[i + 1]].reshape(128, FP)], axis=0)
            term = lax.dot_general(hid[...], w, (((1,), (1,)), ((), ())), preferred_element_type=F32)
            part[k, :, :, :, pl.ds(i * 128, 256)] = term.astype(BF).reshape(NC, NX, OWN, 256)
        chunks[k]["pair"] = send(part.at[k, pc], pair_in.at[k], dev_p)

    def fold(k):
        g = chunks[k]
        g["pair"].wait_recv()
        summed[k] = (part[k, c].astype(F32) + pair_in[k].astype(F32)).astype(BF)
        g["opp_a"] = send(summed.at[k, xo, :, low], opp_in.at[k, 0], dev_xr)
        g["opp_b"] = send(summed.at[k, xo, :, high], opp_in.at[k, 1], dev_xl)
        g["near_b"] = send(summed.at[k, xr, :, high], near_in.at[k, 1], dev_xr)
        g["near_a"] = send(summed.at[k, xl, :, low], near_in.at[k, 0], dev_xl)

    def pass_on(k):
        g = chunks[k]
        g["opp_a"].wait_recv()
        relay[k, 0] = (opp_in[k, 0].astype(F32) + summed[k, xr, :, low].astype(F32)).astype(BF)
        g["far_a"] = send(relay.at[k, 0], far_in.at[k, 0], dev_xr)
        g["opp_b"].wait_recv()
        relay[k, 1] = (opp_in[k, 1].astype(F32) + summed[k, xl, :, high].astype(F32)).astype(BF)
        g["far_b"] = send(relay.at[k, 1], far_in.at[k, 1], dev_xl)

    def slot(k):
        return lambda a, b: shuffled.at[k, b * NX + a]

    def mix(k):
        g = chunks[k]
        base = jnp.concatenate(
            [carried[own, :, pl.ds(pl.multiple_of(at * 128, 128), 128)] for at in groups(k)], axis=1
        ).astype(F32)
        g["near_a"].wait_recv()
        g["near_b"].wait_recv()
        for i, name in ((0, "far_a"), (1, "far_b")):
            g[name].wait_recv()
            cols = pl.ds(i * HALF, HALF)
            feed = summed[k, x, :, cols].astype(F32) + near_in[k, i].astype(F32) + far_in[k, i].astype(F32)
            feed = feed.astype(BF).astype(F32)
            shuffled[k, own, :, cols] = (base[:, i * HALF : (i + 1) * HALF] + 0.5 * feed).astype(BF)
        g["out"] = x_start(shuffled.at[k, own], slot(k))

    def forward(k):
        x_forward(chunks[k]["out"], slot(k), lane_halves)

    def hand_over(k):
        x_relay(chunks[k]["out"], slot(k), lane_halves)

    def write(k):
        x_done(chunks[k]["out"])
        for i, at in enumerate(groups(k)):
            cols = pl.ds(pl.multiple_of(at * 128, 128), 128)
            out[:, :, cols] = shuffled[k, :, :, pl.ds(i * 128, 128)]

    for i in range(1, 7):
        dn.done(i)
    lower(0)
    lower(1)
    fold(0)
    lower(2)
    fold(1)
    dn.done(7)
    dn.done(0)
    dn.done(8)
    lower(3)
    fold(2)
    pass_on(0)
    fold(3)
    pass_on(1)
    mix(0)
    pass_on(2)
    mix(1)
    forward(0)
    pass_on(3)
    mix(2)
    forward(1)
    hand_over(0)
    mix(3)
    forward(2)
    hand_over(1)
    write(0)
    forward(3)
    hand_over(2)
    write(1)
    hand_over(3)
    write(2)
    write(3)
    for copy in started:
        copy.wait_send()


def per_device(
    stream,
    query_rows,
    key_rows,
    value_rows,
    doc_ids,
    sink_logit,
    out_weight,
    norm_gain,
    gate_weight,
    up_weight,
    down_weight,
):
    vmem = pl.BlockSpec(memory_space=pltpu.VMEM)
    smem = pl.BlockSpec(memory_space=pltpu.SMEM)
    far = pl.BlockSpec(memory_space=pltpu.HBM)
    result = pl.pallas_call(
        kernel,
        name="layer",
        out_shape=pltpu.VMEM((8, OWN, D), BF),
        in_specs=[far] * 5 + [smem] + [far] * 5,
        out_specs=vmem,
        scratch_shapes=[
            pltpu.VMEM((TOK, D), BF),
            pltpu.VMEM((TOK, HD), BF),
            pltpu.VMEM((TOK, 2 * HD), BF),
            pltpu.VMEM((TOK, 2 * HD), BF),
            pltpu.VMEM((3, 128), jnp.int32),
            pltpu.VMEM((128, D), BF),
            pltpu.VMEM((1, D), F32),
            pltpu.VMEM((32, FFL), BF),
            pltpu.VMEM((32, FFL), BF),
            pltpu.VMEM((32, FFL), BF),
            pltpu.SemaphoreType.DMA((10,)),
            pltpu.VMEM((TOK + 2 * WIN, HD), BF),
            pltpu.VMEM((TOK + 2 * WIN, HD), BF),
            pltpu.VMEM((2, 8, 128), jnp.int32),
            pltpu.VMEM((2, 8, 128), jnp.int32),
            pltpu.VMEM((32, FP), BF),
            pltpu.VMEM((32, FP), BF),
            pltpu.VMEM((NZ, NY, 32, MAIN), BF),
            pltpu.VMEM((NZ, NY, 32, FP), BF),
            pltpu.VMEM((NZ, NY, 32, FP), BF),
            pltpu.VMEM((8, 128, D), BF),
            pltpu.VMEM((8, TOK, HD), BF),
            pltpu.VMEM((8, OWN, D), BF),
            pltpu.VMEM((TOK, D), BF),
            pltpu.VMEM((TOK, MAIN), F32),
            pltpu.VMEM((TOK, FP), F32),
            pltpu.VMEM((TOK, FP), BF),
            pltpu.VMEM((4, NC, NX, OWN, CHUNK), BF),
            pltpu.VMEM((4, NX, OWN, CHUNK), BF),
            pltpu.VMEM((4, NX, OWN, CHUNK), BF),
            pltpu.VMEM((4, 2, OWN, HALF), BF),
            pltpu.VMEM((4, 2, OWN, HALF), BF),
            pltpu.VMEM((4, 2, OWN, HALF), BF),
            pltpu.VMEM((4, 2, OWN, HALF), BF),
            pltpu.VMEM((4, 8, OWN, CHUNK), BF),
            pltpu.SemaphoreType.DMA((COPIES,)),
            pltpu.SemaphoreType.DMA((COPIES,)),
        ],
        compiler_params=pltpu.CompilerParams(
            collective_id=0, has_side_effects=True, vmem_limit_bytes=60 * 1024 * 1024
        ),
    )(
        stream,
        query_rows,
        key_rows,
        value_rows,
        doc_ids.reshape(3, 128),
        sink_logit,
        out_weight,
        norm_gain.reshape(1, D),
        gate_weight,
        up_weight,
        down_weight.T,
    )
    return result.reshape(TOK, D)


def solution(mesh):
    split = Mesh(mesh.devices.reshape(NZ, NY, NX, NC), ("z", "y", "x", "c"))
    placed = (
        P(SP, None),
        P(SP, TP),
        P(SP, None),
        P(SP, None),
        P(SP),
        P(TP),
        P(TP, None),
        P(),
        P(SP, TP),
        P(SP, TP),
        P(TP, SP),
    )
    return jax.shard_map(
        per_device, mesh=split, in_specs=placed, out_specs=P(SP, None), check_vma=False
    )
```

```python
import jax
import jax.numpy as jnp
from jax import lax
from jax.experimental import pallas as pl
from jax.experimental.pallas import tpu as pltpu
from jax.sharding import Mesh
from jax.sharding import PartitionSpec as P

HD = 128
WIN = 128
NZ, NY, NX, NC = 16, 4, 4, 2
TOK = 384
D = 2048
FFL = 704
MAIN = 640
TAIL = 64
FP = 768
OWN = TOK // (NX * NC)
EPS = 1e-06
LOW = -1e30
COPIES = 280
CHUNK = D // 4
HALF = CHUNK // 2
SP = ("z", "y")
TP = ("x", "c")
F32 = jnp.float32
BF = jnp.bfloat16


def kernel(
    far_stream,
    far_query,
    far_key,
    far_value,
    far_docs,
    sink,
    far_out_w,
    far_gain,
    far_gate_w,
    far_up_w,
    far_down_w,
    out,
    stream,
    query,
    key,
    value,
    docs,
    out_w,
    gain,
    gate_w,
    up_w,
    down_w,
    local_sems,
    kext,
    vext,
    dsend,
    dext,
    gb_own,
    dn_own,
    wga,
    wgb,
    wd,
    ow,
    att,
    carried,
    normed,
    acc_a,
    acc_b,
    hid,
    part,
    summed,
    pair_in,
    opp_in,
    relay,
    near_in,
    far_in,
    shuffled,
    send_sems,
    recv_sems,
):
    z, y = lax.axis_index("z"), lax.axis_index("y")
    x, c = lax.axis_index("x"), lax.axis_index("c")
    zr, zl = lax.rem(z + 1, NZ), lax.rem(z + NZ - 1, NZ)
    yr, yl = lax.rem(y + 1, NY), lax.rem(y + NY - 1, NY)
    xr, xl = lax.rem(x + 1, NX), lax.rem(x + NX - 1, NX)
    yo, xo = lax.rem(y + 2, NY), lax.rem(x + 2, NX)
    pc = 1 - c
    sp = z * NY + y
    after, before = lax.rem(sp + 1, NZ * NY), lax.rem(sp + NZ * NY - 1, NZ * NY)
    dev_zr, dev_zl = (zr, y, x, c), (zl, y, x, c)
    dev_yr, dev_yl = (z, yr, x, c), (z, yl, x, c)
    dev_xr, dev_xl = (z, y, xr, c), (z, y, xl, c)
    dev_p = (z, y, x, pc)
    dev_after = (after // NY, lax.rem(after, NY), x, c)
    dev_before = (before // NY, lax.rem(before, NY), x, c)

    barrier = pltpu.get_barrier_semaphore()
    peers = (dev_zr, dev_zl, dev_yr, dev_yl, dev_xr, dev_xl, dev_p, dev_after, dev_before)
    for peer in peers:
        pl.semaphore_signal(barrier, inc=1, device_id=peer, device_id_type=pl.DeviceIdType.MESH)

    local = {}

    def fetch(name, src, dst):
        local[name] = pltpu.make_async_copy(src, dst, local_sems.at[len(local)])
        local[name].start()

    fetch("gate_w", far_gate_w, gate_w)
    fetch("up_w", far_up_w, up_w)
    fetch("down_w", far_down_w, down_w)
    fetch("docs", far_docs, docs)
    fetch("key", far_key, key)
    fetch("value", far_value, value)
    fetch("out_w", far_out_w, out_w)
    fetch("query", far_query, query)
    fetch("gain", far_gain, gain)
    fetch("stream", far_stream, stream)
    local["gate_w"].wait()
    local["up_w"].wait()
    local["down_w"].wait()
    gb_own[:, 0:MAIN] = up_w[:, 0:MAIN]
    gb_own[:, MAIN:FP] = jnp.concatenate([gate_w[:, MAIN:FFL], up_w[:, MAIN:FFL]], axis=1)
    dn_own[:, 0:MAIN] = down_w[:, 0:MAIN]
    dn_own[:, MAIN:FP] = jnp.concatenate([down_w[:, MAIN:FFL], jnp.zeros((32, TAIL), BF)], axis=1)
    local["docs"].wait()
    dsend[0] = jnp.broadcast_to(docs[2:3], (8, 128))
    dsend[1] = jnp.broadcast_to(docs[0:1], (8, 128))
    group = pl.multiple_of((x // 2) * HD, HD)
    lanes = pl.ds(group, HD)
    local["key"].wait()
    local["value"].wait()
    local["out_w"].wait()
    wga[z, y] = gate_w[:, 0:MAIN]

    pl.semaphore_wait(barrier, len(peers))

    started = []

    def send(src, dst, dev):
        at = len(started)
        copy = pltpu.make_async_remote_copy(
            src_ref=src,
            dst_ref=dst,
            send_sem=send_sems.at[at],
            recv_sem=recv_sems.at[at],
            device_id=dev,
            device_id_type=pl.DeviceIdType.MESH,
        )
        copy.start()
        started.append(copy)
        return copy

    def zm(s):
        return lax.rem(z + NZ - s, NZ)

    def zp(s):
        return lax.rem(z + s, NZ)

    def tags(s):
        if s == 0:
            return [(0, 0)]
        if s == 8:
            return [(0, 8)]
        return [(0, s), (1, s)]

    def place(tag):
        return zm(tag[1]) if tag[0] == 0 else zp(tag[1])

    class ZFirst:
        def __init__(self, own, buf):
            self.own, self.buf = own, buf
            self.left, self.right, self.yl, self.yr, self.yo = {}, {}, {}, {}, {}

        def to_y(self, src, at, tag):
            self.yl[tag] = send(src, self.buf.at[at, y], dev_yr)
            self.yr[tag] = send(src, self.buf.at[at, y], dev_yl)

        def start(self):
            self.left[0] = send(self.own, self.buf.at[z, y], dev_zr)
            self.right[0] = send(self.own, self.buf.at[z, y], dev_zl)
            self.to_y(self.own, z, (0, 0))

        def ring(self, s):
            block = self.buf.at[zm(s), y]
            self.left[s - 1].wait_recv()
            if s < 8:
                self.left[s] = send(block, block, dev_zr)
            if s <= 7:
                block = self.buf.at[zp(s), y]
                self.right[s - 1].wait_recv()
                if s < 7:
                    self.right[s] = send(block, block, dev_zl)
            for tag in tags(s):
                at = place(tag)
                self.to_y(self.buf.at[at, y], at, tag)

        def across(self, s):
            for tag in tags(s):
                at = place(tag)
                rightward = tag[0] == 0 and tag[1] < 8
                self.yl[tag].wait_recv()
                if rightward:
                    self.yo[tag] = send(self.buf.at[at, yl], self.buf.at[at, yl], dev_yr)
                self.yr[tag].wait_recv()
                if not rightward:
                    self.yo[tag] = send(self.buf.at[at, yr], self.buf.at[at, yr], dev_yl)

        def done(self, s):
            for tag in tags(s):
                self.yo[tag].wait_recv()

    class YFirst:
        def __init__(self, own, buf):
            self.own, self.buf = own, buf
            self.left, self.right = {}, {}

        def begin_piece(self, p, col, src):
            self.left[p, 0] = send(src, self.buf.at[z, col], dev_zr)
            self.right[p, 0] = send(src, self.buf.at[z, col], dev_zl)

        def start(self):
            self.from_l = send(self.own, self.buf.at[z, y], dev_yr)
            self.from_r = send(self.own, self.buf.at[z, y], dev_yl)
            self.begin_piece(0, y, self.own)

        def begin(self):
            self.from_l.wait_recv()
            block = self.buf.at[z, yl]
            self.from_o = send(block, block, dev_yr)
            self.begin_piece(1, yl, block)
            self.from_r.wait_recv()
            self.begin_piece(2, yr, self.buf.at[z, yr])

        def begin_last(self):
            self.from_o.wait_recv()
            self.begin_piece(3, yo, self.buf.at[z, yo])

        def ring(self, s):
            for p, col in enumerate((y, yl, yr, yo)):
                self.left[p, s - 1].wait_recv()
                if s < 8:
                    block = self.buf.at[zm(s), col]
                    self.left[p, s] = send(block, block, dev_zr)
                if s <= 7:
                    self.right[p, s - 1].wait_recv()
                    if s < 7:
                        block = self.buf.at[zp(s), col]
                        self.right[p, s] = send(block, block, dev_zl)

    def x_start(src, slot):
        own = slot(x, c)
        return {"l": send(src, own, dev_xr), "r": send(src, own, dev_xl), "p": send(src, own, dev_p)}

    def x_forward(g, slot, halves):
        left, right = slot(xl, c), slot(xr, c)
        g["l"].wait_recv()
        g["a"] = send(halves(left)[0], halves(left)[0], dev_xr)
        g["pl"] = send(left, left, dev_p)
        g["r"].wait_recv()
        g["b"] = send(halves(right)[1], halves(right)[1], dev_xl)
        g["pr"] = send(right, right, dev_p)

    def x_relay(g, slot, halves):
        a, b = halves(slot(xo, c))
        g["a"].wait_recv()
        g["pa"] = send(a, a, dev_p)
        g["b"].wait_recv()
        g["pb"] = send(b, b, dev_p)

    def x_done(g):
        for name in ("p", "pl", "pr", "pa", "pb"):
            g[name].wait_recv()

    def ow_slot(a, b):
        return ow.at[a * NC + b]

    def ow_halves(ref):
        return ref.at[pl.ds(0, 64)], ref.at[pl.ds(64, 64)]

    def att_slot(a, b):
        return att.at[a * NC + b]

    def att_halves(ref):
        return ref.at[pl.ds(0, 192)], ref.at[pl.ds(192, 192)]

    def lane_halves(ref):
        return ref.at[:, pl.ds(0, HALF)], ref.at[:, pl.ds(HALF, HALF)]

    ga = ZFirst(gate_w.at[:, pl.ds(0, MAIN)], wga)
    gb = YFirst(gb_own, wgb)
    dn = ZFirst(dn_own, wd)
    gb.start()
    ga.start()
    dn.start()
    halo = [
        send(key.at[pl.ds(256, 128), lanes], kext.at[pl.ds(0, 128)], dev_after),
        send(value.at[pl.ds(256, 128), lanes], vext.at[pl.ds(0, 128)], dev_after),
        send(dsend.at[0], dext.at[0], dev_after),
        send(key.at[pl.ds(0, 128), lanes], kext.at[pl.ds(512, 128)], dev_before),
        send(value.at[pl.ds(0, 128), lanes], vext.at[pl.ds(512, 128)], dev_before),
        send(dsend.at[1], dext.at[1], dev_before),
    ]
    ow_g = x_start(out_w, ow_slot)
    ow[x * NC + c] = out_w[...]
    wgb[z, y] = gb_own[...]
    wd[z, y] = dn_own[...]
    kext[pl.ds(128, 384), :] = key[:, lanes]
    vext[pl.ds(128, 384), :] = value[:, lanes]
    local["query"].wait()
    gb.begin()

    def attend(block):
        q = query[pl.ds(block * 128, 128), :]
        k = kext[pl.ds(block * 128, 384), :]
        v = vext[pl.ds(block * 128, 384), :]
        scores = lax.dot_general(q, k, (((1,), (1,)), ((), ())), preferred_element_type=F32)
        scores = scores * HD ** (-0.5)
        if block == 0:
            first = jnp.where(sp == 0, -1, dext[0, 0:1])
        else:
            first = docs[block - 1 : block]
        if block == 2:
            last = jnp.where(sp == NZ * NY - 1, -1, dext[1, 0:1])
        else:
            last = docs[block + 1 : block + 2]
        around = jnp.concatenate([first, docs[block : block + 1], last], axis=1)
        mine = jnp.transpose(jnp.broadcast_to(docs[block : block + 1], (128, 128)))[:, 0:1]
        row = lax.broadcasted_iota(jnp.int32, (128, 384), 0)
        col = lax.broadcasted_iota(jnp.int32, (128, 384), 1)
        allowed = (col >= row) & (col <= row + 2 * WIN) & (mine == around)
        masked = jnp.where(allowed, scores, LOW)
        here = sink[0]
        peak = jnp.maximum(jnp.max(masked, axis=1, keepdims=True), here)
        lifted = jnp.where(allowed, jnp.exp(masked - peak), 0.0)
        denom = jnp.sum(lifted, axis=1, keepdims=True) + jnp.exp(here - peak)
        probs = (lifted / denom).astype(BF)
        attended = jnp.dot(probs, v, preferred_element_type=F32).astype(BF)
        att[x * NC + c, pl.ds(block * 128, 128), :] = attended

    def rings(s):
        ga.ring(s)
        ga.across(s - 1)
        dn.ring(s)
        dn.across(s - 1)
        gb.ring(s)

    attend(1)
    gb.begin_last()
    for copy in halo:
        copy.wait_recv()
    attend(0)
    rings(1)
    attend(2)
    rings(2)
    att_g = x_start(att.at[x * NC + c], att_slot)
    x_forward(ow_g, ow_slot, ow_halves)
    rings(3)
    x_forward(att_g, att_slot, att_halves)
    x_relay(ow_g, ow_slot, ow_halves)
    x_relay(att_g, att_slot, att_halves)
    rings(4)
    x_done(ow_g)
    x_done(att_g)

    local["gain"].wait()
    local["stream"].wait()

    def project(n, squares):
        cols = pl.ds(pl.multiple_of(n * 256, 256), 256)
        left = jnp.concatenate([att[h] for h in range(8)], axis=1)
        right = ow[:, :, cols].reshape(1024, 256)
        branch = jnp.dot(left, right, preferred_element_type=F32).astype(BF)
        total = (stream[:, cols].astype(F32) + branch.astype(F32)).astype(BF)
        carried[:, :, cols] = total.reshape(8, OWN, 256)
        wide = total.astype(F32)
        return squares + jnp.sum(wide * wide, axis=1, keepdims=True)

    squares = lax.fori_loop(0, 8, project, jnp.zeros((TOK, 1), F32))
    scale = lax.rsqrt(squares / D + EPS)

    rings(5)

    def normalize(n, carry):
        cols = pl.ds(pl.multiple_of(n * 256, 256), 256)
        wide = carried[:, :, cols].reshape(TOK, 256).astype(F32)
        normed[:, cols] = (wide * scale * gain[:, cols]).astype(BF)
        return carry

    lax.fori_loop(0, 8, normalize, 0)

    def accumulate(za, zb, first):
        left = jnp.concatenate(
            [
                normed[:, pl.ds(pl.multiple_of(za * 128, 128), 128)],
                normed[:, pl.ds(pl.multiple_of(zb * 128, 128), 128)],
            ],
            axis=1,
        )
        for buf, acc, width in ((wga, acc_a, MAIN), (wgb, acc_b, FP)):
            right = jnp.concatenate([buf[za].reshape(128, width), buf[zb].reshape(128, width)], axis=0)
            term = jnp.dot(left, right, preferred_element_type=F32)
            if first:
                acc[...] = term
            else:
                acc[...] += term

    def accumulate_tag(s, first=False):
        accumulate(zm(s), zp(s), first)

    ga.done(1)
    accumulate_tag(1, True)
    rings(6)
    ga.done(2)
    ga.done(3)

    def both(i, carry):
        accumulate_tag(i)
        return carry

    lax.fori_loop(2, 4, both, 0)
    rings(7)
    ga.done(4)
    accumulate_tag(4)
    rings(8)
    ga.done(5)
    accumulate_tag(5)
    ga.done(6)
    accumulate_tag(6)
    ga.across(8)
    dn.across(8)
    ga.done(7)
    accumulate_tag(7)
    ga.done(0)
    ga.done(8)
    accumulate(z, zm(8), False)

    gate, up = acc_a[...], acc_b[:, 0:MAIN]
    hid[:, 0:MAIN] = (gate / (1.0 + jnp.exp(-gate)) * up).astype(BF)
    rest = acc_b[:, MAIN:FP]
    swapped = pltpu.roll(rest, TAIL, 1)
    tail = rest / (1.0 + jnp.exp(-rest)) * swapped
    lane = lax.broadcasted_iota(jnp.int32, (TOK, 2 * TAIL), 1)
    hid[:, MAIN:FP] = jnp.where(lane < TAIL, tail, 0.0).astype(BF)

    own = c * NX + x
    low, high = pl.ds(0, HALF), pl.ds(HALF, HALF)
    chunks = [{} for _ in range(4)]

    def groups(k):
        if k == 3:
            return [zm(7), zp(7), z, zm(8)]
        return [zm(2 * k + 1), zp(2 * k + 1), zm(2 * k + 2), zp(2 * k + 2)]

    def lower(k):
        at = groups(k)
        for i in (0, 2):
            w = jnp.concatenate([wd[at[i]].reshape(128, FP), wd[at[i + 1]].reshape(128, FP)], axis=0)
            term = lax.dot_general(hid[...], w, (((1,), (1,)), ((), ())), preferred_element_type=F32)
            part[k, :, :, :, pl.ds(i * 128, 256)] = term.astype(BF).reshape(NC, NX, OWN, 256)
        chunks[k]["pair"] = send(part.at[k, pc], pair_in.at[k], dev_p)

    def fold(k):
        g = chunks[k]
        g["pair"].wait_recv()
        summed[k] = (part[k, c].astype(F32) + pair_in[k].astype(F32)).astype(BF)
        g["opp_a"] = send(summed.at[k, xo, :, low], opp_in.at[k, 0], dev_xr)
        g["opp_b"] = send(summed.at[k, xo, :, high], opp_in.at[k, 1], dev_xl)
        g["near_b"] = send(summed.at[k, xr, :, high], near_in.at[k, 1], dev_xr)
        g["near_a"] = send(summed.at[k, xl, :, low], near_in.at[k, 0], dev_xl)

    def pass_on(k):
        g = chunks[k]
        g["opp_a"].wait_recv()
        relay[k, 0] = (opp_in[k, 0].astype(F32) + summed[k, xr, :, low].astype(F32)).astype(BF)
        g["far_a"] = send(relay.at[k, 0], far_in.at[k, 0], dev_xr)
        g["opp_b"].wait_recv()
        relay[k, 1] = (opp_in[k, 1].astype(F32) + summed[k, xl, :, high].astype(F32)).astype(BF)
        g["far_b"] = send(relay.at[k, 1], far_in.at[k, 1], dev_xl)

    def slot(k):
        return lambda a, b: shuffled.at[k, b * NX + a]

    def mix(k):
        g = chunks[k]
        base = jnp.concatenate(
            [carried[own, :, pl.ds(pl.multiple_of(at * 128, 128), 128)] for at in groups(k)], axis=1
        ).astype(F32)
        g["near_a"].wait_recv()
        g["near_b"].wait_recv()
        for i, name in ((0, "far_a"), (1, "far_b")):
            g[name].wait_recv()
            cols = pl.ds(i * HALF, HALF)
            feed = summed[k, x, :, cols].astype(F32) + near_in[k, i].astype(F32) + far_in[k, i].astype(F32)
            feed = feed.astype(BF).astype(F32)
            shuffled[k, own, :, cols] = (base[:, i * HALF : (i + 1) * HALF] + 0.5 * feed).astype(BF)
        g["out"] = x_start(shuffled.at[k, own], slot(k))

    def forward(k):
        x_forward(chunks[k]["out"], slot(k), lane_halves)

    def hand_over(k):
        x_relay(chunks[k]["out"], slot(k), lane_halves)

    def write(k):
        x_done(chunks[k]["out"])
        for i, at in enumerate(groups(k)):
            cols = pl.ds(pl.multiple_of(at * 128, 128), 128)
            out[:, :, cols] = shuffled[k, :, :, pl.ds(i * 128, 128)]

    for i in range(1, 7):
        dn.done(i)
    lower(0)
    lower(1)
    fold(0)
    lower(2)
    fold(1)
    dn.done(7)
    dn.done(0)
    dn.done(8)
    lower(3)
    pass_on(0)
    fold(2)
    fold(3)
    pass_on(1)
    mix(0)
    pass_on(2)
    mix(1)
    forward(0)
    pass_on(3)
    mix(2)
    forward(1)
    hand_over(0)
    mix(3)
    forward(2)
    hand_over(1)
    write(0)
    forward(3)
    hand_over(2)
    write(1)
    hand_over(3)
    write(2)
    write(3)
    for copy in started:
        copy.wait_send()


def per_device(
    stream,
    query_rows,
    key_rows,
    value_rows,
    doc_ids,
    sink_logit,
    out_weight,
    norm_gain,
    gate_weight,
    up_weight,
    down_weight,
):
    vmem = pl.BlockSpec(memory_space=pltpu.VMEM)
    smem = pl.BlockSpec(memory_space=pltpu.SMEM)
    far = pl.BlockSpec(memory_space=pltpu.HBM)
    result = pl.pallas_call(
        kernel,
        name="layer",
        out_shape=pltpu.VMEM((8, OWN, D), BF),
        in_specs=[far] * 5 + [smem] + [far] * 5,
        out_specs=vmem,
        scratch_shapes=[
            pltpu.VMEM((TOK, D), BF),
            pltpu.VMEM((TOK, HD), BF),
            pltpu.VMEM((TOK, 2 * HD), BF),
            pltpu.VMEM((TOK, 2 * HD), BF),
            pltpu.VMEM((3, 128), jnp.int32),
            pltpu.VMEM((128, D), BF),
            pltpu.VMEM((1, D), F32),
            pltpu.VMEM((32, FFL), BF),
            pltpu.VMEM((32, FFL), BF),
            pltpu.VMEM((32, FFL), BF),
            pltpu.SemaphoreType.DMA((10,)),
            pltpu.VMEM((TOK + 2 * WIN, HD), BF),
            pltpu.VMEM((TOK + 2 * WIN, HD), BF),
            pltpu.VMEM((2, 8, 128), jnp.int32),
            pltpu.VMEM((2, 8, 128), jnp.int32),
            pltpu.VMEM((32, FP), BF),
            pltpu.VMEM((32, FP), BF),
            pltpu.VMEM((NZ, NY, 32, MAIN), BF),
            pltpu.VMEM((NZ, NY, 32, FP), BF),
            pltpu.VMEM((NZ, NY, 32, FP), BF),
            pltpu.VMEM((8, 128, D), BF),
            pltpu.VMEM((8, TOK, HD), BF),
            pltpu.VMEM((8, OWN, D), BF),
            pltpu.VMEM((TOK, D), BF),
            pltpu.VMEM((TOK, MAIN), F32),
            pltpu.VMEM((TOK, FP), F32),
            pltpu.VMEM((TOK, FP), BF),
            pltpu.VMEM((4, NC, NX, OWN, CHUNK), BF),
            pltpu.VMEM((4, NX, OWN, CHUNK), BF),
            pltpu.VMEM((4, NX, OWN, CHUNK), BF),
            pltpu.VMEM((4, 2, OWN, HALF), BF),
            pltpu.VMEM((4, 2, OWN, HALF), BF),
            pltpu.VMEM((4, 2, OWN, HALF), BF),
            pltpu.VMEM((4, 2, OWN, HALF), BF),
            pltpu.VMEM((4, 8, OWN, CHUNK), BF),
            pltpu.SemaphoreType.DMA((COPIES,)),
            pltpu.SemaphoreType.DMA((COPIES,)),
        ],
        compiler_params=pltpu.CompilerParams(
            collective_id=0, has_side_effects=True, vmem_limit_bytes=60 * 1024 * 1024
        ),
    )(
        stream,
        query_rows,
        key_rows,
        value_rows,
        doc_ids.reshape(3, 128),
        sink_logit,
        out_weight,
        norm_gain.reshape(1, D),
        gate_weight,
        up_weight,
        down_weight.T,
    )
    return result.reshape(TOK, D)


def solution(mesh):
    split = Mesh(mesh.devices.reshape(NZ, NY, NX, NC), ("z", "y", "x", "c"))
    placed = (
        P(SP, None),
        P(SP, TP),
        P(SP, None),
        P(SP, None),
        P(SP),
        P(TP),
        P(TP, None),
        P(),
        P(SP, TP),
        P(SP, TP),
        P(TP, SP),
    )
    return jax.shard_map(
        per_device, mesh=split, in_specs=placed, out_specs=P(SP, None), check_vma=False
    )
```
